32 devices in a mesh: gr: 2 (over x), fs: 8 (over z, y), tp: 2 (over core).
Axes of the slice: x: 2, y: 2, z: 4, core: 2. Of those that a mesh axis runs over, the one named last changes fastest.
Arguments:
- tokens: bfloat16 [2048, 2048], P(('gr', 'tp')), may hold values from -6 to 6
- norm_gain: float32 [2048], P('fs'), may hold values from 0.1 to 1.9
- up_weight: float32 [2048, 8192], P('fs', ('gr', 'tp')), may hold values from -0.125 to 0.125
- down_weight: float32 [8192, 2048], P('fs', ('gr', 'tp')), may hold values from -0.09375 to 0.09375
Outputs:
- sampler_up: bfloat16 [2048, 8192], P(None, 'fs')
- sampler_down: bfloat16 [8192, 2048], P('fs')
- mixed: bfloat16 [2048, 2048], P(('gr', 'tp'), 'fs')
The draws below stay inside these ranges and needn't reach their ends.
All inputs are finite; a program needn't handle non-finite values.
Results may differ from the reference program's by a relative error of at most 0.023.
Values may be sent and summed in bfloat16 or wider, within the bound.
A program may use at most 64 MiB of HBM per device.

```python
import jax
import jax.numpy as jnp
from jax import lax

D = 2048
FF = 8192
ROWS = 2048
N_FS = 8


def spiked(drawn, stream_key, source, target, blocks, factor):
    owner, partner = [(jnp.arange(drawn.shape[position]) // (drawn.shape[position] // blocks)).reshape([-1 if axis == position else 1 for axis in range(drawn.ndim)]) for position in (source, target)]
    chosen = jax.random.permutation(stream_key, blocks)[partner]
    strong = (owner == chosen) | (owner == (partner + blocks // 2) % blocks)
    return jnp.where(strong, factor * drawn, drawn)


def block_levels(rng, shape, cuts, smallest, top_value):
    gain, own = 1.0, jax.random.fold_in(rng, 6)
    for axis_at, blocks in cuts:
        draws = jnp.exp(jax.random.uniform(jax.random.fold_in(own, axis_at), (blocks,), jnp.float32, smallest / len(cuts), top_value / len(cuts)))
        gain = gain * jnp.repeat(draws, shape[axis_at] // blocks).reshape([-1 if axis == axis_at else 1 for axis in range(len(shape))])
    return gain


def bell_draw(key, extent, deviation, bound, cuts=(), held_as=jnp.bfloat16):
    result = jax.random.normal(key, extent, jnp.float32) * deviation
    if len(cuts) > 0:
        result = block_levels(key, extent, cuts, -0.22, 0.18) * result
    return jnp.clip(result, min=-bound, max=bound).astype(held_as)


def heavy_noise(own_key, dims, spread, limit, shards, heavy, held_as=jnp.bfloat16):
    entries = spread * jax.random.normal(own_key, dims, jnp.float32)
    if shards:
        entries = entries * block_levels(own_key, dims, shards, -0.22, 0.18)
    return jnp.clip(spiked(entries, jax.random.fold_in(own_key, 3), *heavy), -limit, limit).astype(held_as)


def setup_inputs(seed: int = 0) -> dict:
    streams_of = jax.random.split(jax.random.key(seed), 5)
    tokens = bell_draw(streams_of[0], (ROWS, D), 1.0, 6.0, ((0, 4),))
    norm_gain = jnp.clip(1.0 + 0.18 * jax.random.normal(streams_of[1], (D,), jnp.float32), 0.1, 1.9)
    up_weight = bell_draw(streams_of[2], (D, FF), D ** -0.5, 0.125, ((0, 8), (1, 4)), jnp.float32)
    down_weight = heavy_noise(streams_of[3], (FF, D), FF ** -0.5, 0.09375, ((0, 8), (1, 4)), (0, 1, 8, 2.0), jnp.float32)
    return dict(tokens=tokens, norm_gain=norm_gain, up_weight=up_weight, down_weight=down_weight)


def reference(tokens, norm_gain, up_weight, down_weight):
    sampler_up = (norm_gain[:, None] * up_weight).astype(jnp.bfloat16)
    sampler_down = down_weight.astype(jnp.bfloat16)
    widened = tokens.astype(jnp.float32)
    normed = (widened * lax.rsqrt(lax.optimization_barrier(jnp.mean(widened * widened, axis=-1, keepdims=True)) + 1e-06)).astype(jnp.bfloat16)
    preact = jnp.dot(normed, sampler_up, preferred_element_type=jnp.float32)
    hidden = jnp.square(jax.nn.relu(preact)).astype(jnp.bfloat16)
    block_units = FF // N_FS

    def add_block(total, index):
        begin = (index * block_units).astype(jnp.int32)
        hidden_part = lax.dynamic_slice_in_dim(hidden, begin, block_units, 1)
        down_part = lax.dynamic_slice_in_dim(sampler_down, begin, block_units, 0)
        partial_value = jnp.dot(hidden_part, down_part, preferred_element_type=jnp.float32).astype(jnp.bfloat16)
        partial_value = lax.optimization_barrier(partial_value)
        return (total + partial_value.astype(jnp.float32), None)
    start_total = jnp.zeros((tokens.shape[0], D), jnp.float32)
    summed, _ = lax.scan(add_block, start_total, jnp.arange(N_FS, dtype=jnp.int32))
    return (sampler_up, sampler_down, summed.astype(jnp.bfloat16))
```

```python
import functools

import jax
import jax.numpy as jnp
from jax import lax
from jax.experimental import pallas as pl
from jax.experimental.pallas import tpu as pltpu
from jax.sharding import PartitionSpec as P

MESH = pl.DeviceIdType.MESH
MIB = 1024 * 1024
FUSED_VMEM = 36
COPY_VMEM = 4
SLICE_ROWS = 32
SINGLE_NUM, SINGLE_DEN = 1, 4
PIECES = 4
DOWN_CHUNKS = 2
COPY_CHUNKS = 4


def flipped(index, step, count):
    if count & (count - 1):
        return lax.rem(index + step, count)
    bit = 1
    while bit < count:
        if step & bit:
            index = index + (1 - 2 * lax.rem(index // bit, 2)) * bit
        bit *= 2
    return index


def remote(src, dst, send, recv, device):
    return pltpu.make_async_remote_copy(
        src_ref=src, dst_ref=dst, send_sem=send, recv_sem=recv,
        device_id=device, device_id_type=MESH,
    )


def when_not(condition):
    return pl.when(jnp.logical_not(condition))


def fused_kernel(
    tp, blocks, shards, single, tokens_in, gain_in, up_in, down_in, up_out, down_out, mixed,
    tokens, gain, up, down, loads, gath, normed, acc, hidden, part, ybuf, zout, zin,
    xs, xr, fsend, frecv, msend, ps, pr, ods, odr, xds, xdr, pds, pdr, ys, yr, zs, zr,
):
    load = [
        pltpu.make_async_copy(source, kept, loads.at[i])
        for i, (source, kept) in enumerate(
            [(gain_in, gain), (up_in, up), (down_in, down), (tokens_in, tokens)]
        )
    ]
    for copy in load:
        copy.start()
    g, f, t = lax.axis_index("gr"), lax.axis_index("fs"), lax.axis_index("tp")
    per = tp // 2
    chips = gath.shape[0]
    c, k = g * per + t // 2, lax.rem(t, 2)
    rows, width = up.shape
    half = rows // 2
    block = width // blocks
    cols = down.shape[1]
    pairs = ybuf.shape[0]
    wide = mixed.shape[1]
    z, y = f // 2, lax.rem(f, 2)

    def dev(chip, shard, core):
        return (chip // per, shard, lax.rem(chip, per) * 2 + core)

    def down_cols(pair):
        return pl.ds(pl.multiple_of(pair * cols, cols), cols)

    barrier = pltpu.get_barrier_semaphore()
    for s in range(1, chips):
        pl.semaphore_signal(
            barrier, inc=1, device_id=dev(lax.rem(c + s, chips), f, k), device_id_type=MESH
        )
    for s in range(shards):
        for core in range(2):
            if s == 0 and core == 0:
                continue
            other = lax.rem(f + s, shards)
            core_id = lax.rem(k + core, 2)
            pl.semaphore_signal(
                barrier, inc=1, device_id=dev(c, other, core_id), device_id_type=MESH
            )

    load[0].wait()
    square = (rows, rows)
    diagonal = lax.broadcasted_iota(jnp.int32, square, 0) == lax.broadcasted_iota(jnp.int32, square, 1)
    column = jnp.sum(jnp.where(diagonal, gain[...], 0.0), axis=1, keepdims=True)
    load[1].wait()
    gath[c] = (column * up[...]).astype(jnp.bfloat16)
    pl.semaphore_wait(barrier, chips - 1 + 2 * shards - 1)

    slices = xs.shape[2] // 2
    piece = half // slices

    def route(u):
        q = u % slices
        return 1 if q < single else 0 if q < 2 * single else None

    def crosses(source, target):
        return source // (shards // 2) != target // (shards // 2)

    def unit(chip, j, u):
        return gath.at[chip, pl.ds(u * piece, piece), pl.ds(j * block, block)]

    def half_rows(shard, core, first=0, count=half):
        at = pl.multiple_of(shard * rows + core * half + first, piece)
        return up_out.at[pl.ds(at, count), :]

    def target(chip, j):
        return (chip * 2 + k) * blocks + j

    def landing(u):
        return up_out.at[pl.ds(pl.multiple_of(f * rows + u * piece, piece), piece), :]

    def stays(chip, j, u):
        return jnp.logical_and(target(chip, j) == f, k == u // slices)

    def forward(chip, j, u):
        to = target(chip, j)
        at = f if route(u) is None else f + jnp.where(crosses(f, to), shards, 0)
        return remote(
            unit(chip, j, u), landing(u), fsend.at[chip, j, u], frecv.at[at], dev(c, to, u // slices)
        )

    def start_forward(chip, j, u):
        @when_not(stays(chip, j, u))
        def _():
            forward(chip, j, u).start()

        @pl.when(stays(chip, j, u))
        def _():
            landing(u)[...] = unit(chip, j, u)[...]

    def goes(chip, j, u, offset, action):
        if route(u) is None or route(u) == offset:
            action()
        else:
            when_not(crosses(f, target(chip, j)))(action)

    def exchange(s, j, u):
        return remote(
            unit(c, j, u), unit(c, j, u), xs.at[s, j, u], xr.at[s, j, u],
            dev(lax.rem(c + s, chips), f, k),
        )

    def exchanged(s, j, u):
        source = lax.rem(c + chips - s, chips)
        return remote(
            unit(source, j, u), unit(source, j, u), xs.at[s, j, u], xr.at[s, j, u], dev(c, f, k)
        )

    units = [
        [(j, q + core * slices) for core in range(2) for j in range(blocks)] for q in range(slices)
    ]
    for group in units:
        for j, u in group:
            for s in range(1, chips):
                goes(c, j, u, s, lambda: exchange(s, j, u).start())
            goes(c, j, u, 0, lambda: start_forward(c, j, u))

    load[2].wait()
    own_pair = c * 2 + k
    down_out[:, down_cols(own_pair)] = down[...].astype(jnp.bfloat16)
    down_half = down.shape[0] // 2
    chunks = xds.shape[2]
    chunk = down_half // chunks

    def down_own(core):
        held = down_out.at[:, down_cols(c * 2 + core)]
        return remote(held, held, ods.at[0], odr.at[0], dev(c, f, 1 - k))

    down_own(k).start()

    def pair_of(chip, position):
        low = 2 * chip
        return low + jnp.where(z <= low, 1 - position, position)

    def down_piece(pair, core, i):
        at = pl.multiple_of(core * down_half + i * chunk, chunk)
        return down_out.at[pl.ds(at, chunk), down_cols(pair)]

    def down_across(s, position, i):
        held = down_piece(pair_of(c, position), k, i)
        return remote(
            held, held, xds.at[s, position, i], xdr.at[s, position, i],
            dev(lax.rem(c + s, chips), f, k),
        )

    def down_relay(s, position, i, core):
        held = down_piece(pair_of(lax.rem(c + chips - s, chips), position), core, i)
        return remote(held, held, pds.at[s, position, i], pdr.at[s, position, i], dev(c, f, 1 - k))

    def down_arrival(s, position, i):
        held = down_piece(pair_of(lax.rem(c + chips - s, chips), position), k, i)
        return remote(held, held, xds.at[s, position, i], xdr.at[s, position, i], dev(c, f, k))

    load[3].wait()
    widened = tokens[...].astype(jnp.float32)
    scale = lax.rsqrt(jnp.mean(widened * widened, axis=-1, keepdims=True) + 1e-06)
    for shard in range(shards):
        share = tokens[:, shard * rows:(shard + 1) * rows].astype(jnp.float32)
        normed[shard] = (share * scale).astype(jnp.bfloat16)

    owner = f // (2 * blocks)
    offset = lax.rem(c + chips - owner, chips)
    lone = single * piece

    def alone(shard):
        return jnp.logical_and(crosses(shard, f), offset < 2)

    def lone_rows(shard):
        return half_rows(shard, k, (1 - offset) * lone, lone)

    def lone_arrival(shard):
        return remote(
            lone_rows(shard), lone_rows(shard), msend.at[shard, 0], frecv.at[shards + shard], dev(c, f, k)
        )

    def lone_relay(shard, s):
        return remote(
            lone_rows(shard), lone_rows(shard), msend.at[shard, s], frecv.at[shard],
            dev(lax.rem(c + s, chips), f, k),
        )

    even = not shards & (shards - 1)
    far = [s for s in range(1, shards) if single and (not even or s & (shards // 2))]

    def relay_lone():
        for step in far:
            shard = flipped(f, step, shards)

            @pl.when(alone(shard))
            def _():
                lone_arrival(shard).wait_recv()
                for s in range(1, chips):
                    lone_relay(shard, s).start()

    def send_down():
        down_own(1 - k).wait_recv()
        for position in range(2):
            for i in range(chunks):
                for s in range(1, chips):
                    down_across(s, position, i).start()

    for q, group in enumerate(units):
        if q == max(0, slices - 1):
            relay_lone()
            send_down()
        for j, u in group:
            for s in range(1, chips):
                source = lax.rem(c + chips - s, chips)

                def pass_on():
                    exchanged(s, j, u).wait_recv()
                    start_forward(source, j, u)

                goes(source, j, u, s, pass_on)

    source_core = lax.rem(f // blocks, 2)
    own_stays = source_core == k

    def arrive(shard, step):
        def arrival(count):
            held = half_rows(shard, k, 0, count)
            return remote(held, held, ps.at[shard], frecv.at[shard], dev(c, f, 1 - k))

        if step in far:
            @pl.when(alone(shard))
            def _():
                arrival(half - lone).wait_recv()

            @when_not(alone(shard))
            def _():
                arrival(half).wait_recv()
        elif step == 0:
            @when_not(own_stays)
            def _():
                arrival(half).wait_recv()
        else:
            arrival(half).wait_recv()

    def relay(shard, core):
        held = half_rows(shard, core)
        return remote(held, held, ps.at[shard], pr.at[shard], dev(c, f, 1 - k))

    def accumulate(shard, first):
        weights = up_out[pl.ds(pl.multiple_of(shard * rows, rows), rows), :]
        product = jnp.dot(normed[shard], weights, preferred_element_type=jnp.float32)
        if first:
            acc[...] = product
        else:
            acc[...] += product

    near = shards // 2
    steps = list(range(1, near)) + [0] + list(range(near, shards))
    order = [flipped(f, s, shards) for s in steps]
    for position, shard in enumerate(order):
        arrive(shard, steps[position])
        relay(shard, k).start()
        if position > 0:
            before = order[position - 1]
            relay(before, 1 - k).wait_recv()
            accumulate(before, position == 1)
    relay(order[-1], 1 - k).wait_recv()
    accumulate(order[-1], False)
    hidden[...] = jnp.square(jnp.maximum(acc[...], 0.0)).astype(jnp.bfloat16)

    pieces = ys.shape[1]
    span = mixed.shape[0] // pieces

    def across(pair, i):
        at = pl.ds(i * span, span)
        return remote(
            part.at[2 * pair + 1 - y, at], ybuf.at[pair, at], ys.at[pair, i], yr.at[pair, i],
            dev(c, z * 2 + 1 - y, k),
        )

    def along(pair, i):
        at = pl.ds(i * span, span)
        to = z + jnp.where(pair > z, 1, -1)
        slot = jnp.where(jnp.logical_and(pair < z, pair == to), pairs, pair)
        return remote(
            zout.at[pair, at], zin.at[slot, at], zs.at[pair, i], zr.at[slot, i], dev(c, to * 2 + y, k)
        )

    def carried(slot, i):
        held = zin.at[slot, pl.ds(i * span, span)]
        return remote(held, held, zs.at[0, i], zr.at[slot, i], dev(c, f, k))

    def multiply(pair):
        both = jnp.dot(
            hidden[...], down_out[:, down_cols(pair)], preferred_element_type=jnp.float32
        ).astype(jnp.bfloat16)
        part[2 * pair] = both[:, :wide]
        part[2 * pair + 1] = both[:, wide:]
        for i in range(pieces):
            across(pair, i).start()

    def reduce(pair):
        inner = jnp.logical_and(pair != z, jnp.where(pair > z, z > 0, z < pairs - 1))
        outer = jnp.logical_and(pair != z, jnp.logical_not(inner))
        for i in range(pieces):
            at = pl.ds(i * span, span)

            def wide_of(ref, slot):
                return ref[slot, at].astype(jnp.float32)

            def summed():
                return wide_of(part, 2 * pair + y) + wide_of(ybuf, pair)

            across(pair, i).wait_recv()

            @pl.when(inner)
            def _():
                carried(pair, i).wait_recv()
                zout[pair, at] = (summed() + wide_of(zin, pair)).astype(jnp.bfloat16)
                along(pair, i).start()

            @pl.when(outer)
            def _():
                zout[pair, at] = summed().astype(jnp.bfloat16)
                along(pair, i).start()

            @pl.when(pair == z)
            def _():
                @pl.when(z == 0)
                def _():
                    carried(pairs, i).wait_recv()
                    mixed[at] = (summed() + wide_of(zin, pairs)).astype(jnp.bfloat16)

                @pl.when(z == pairs - 1)
                def _():
                    carried(pair, i).wait_recv()
                    mixed[at] = (summed() + wide_of(zin, pair)).astype(jnp.bfloat16)

                @pl.when(jnp.logical_and(z > 0, z < pairs - 1))
                def _():
                    carried(pair, i).wait_recv()
                    carried(pairs, i).wait_recv()
                    total = summed() + wide_of(zin, pair) + wide_of(zin, pairs)
                    mixed[at] = total.astype(jnp.bfloat16)

    def fetch(s, position):
        for i in range(chunks):
            down_arrival(s, position, i).wait_recv()
            down_relay(s, position, i, k).start()
        for i in range(chunks):
            down_relay(s, position, i, 1 - k).wait_recv()

    sequence = [
        (s, position, pair_of(lax.rem(c + chips - s, chips), position))
        for s in range(chips) for position in range(2)
    ]
    ahead = 3
    for i, (s, position, pair) in enumerate(sequence):
        if s > 0:
            fetch(s, position)
        multiply(pair)
        if i >= ahead - 1:
            reduce(sequence[i - ahead + 1][2])
    for _, _, pair in sequence[len(sequence) - ahead + 1:]:
        reduce(pair)

    down_own(k).wait_send()
    for s in range(1, chips):
        for position in range(2):
            for i in range(chunks):
                down_across(s, position, i).wait_send()
                down_relay(s, position, i, k).wait_send()
    for step in far:
        shard = flipped(f, step, shards)

        @pl.when(alone(shard))
        def _():
            for s in range(1, chips):
                lone_relay(shard, s).wait_send()
    for group in units:
        for j, u in group:
            for s in range(1, chips):
                goes(c, j, u, s, lambda: exchange(s, j, u).wait_send())
            for s in range(chips):
                source = lax.rem(c + chips - s, chips)

                def sent():
                    @when_not(stays(source, j, u))
                    def _():
                        forward(source, j, u).wait_send()

                goes(source, j, u, s, sent)
    for shard in order:
        relay(shard, k).wait_send()
    for _, _, pair in sequence:
        for i in range(pieces):
            across(pair, i).wait_send()

            @pl.when(pair != z)
            def _():
                along(pair, i).wait_send()


def copy_kernel(up, down, mixed, up_out, down_out, mixed_out, sems):
    copies = []
    for index, (source, kept) in enumerate([(up, up_out), (down, down_out), (mixed, mixed_out)]):
        count = sems.shape[1]
        span = source.shape[0] // count
        for i in range(count):
            at = pl.ds(i * span, span)
            copies.append(pltpu.make_async_copy(source.at[at], kept.at[at], sems.at[index, i]))
    for copy in copies:
        copy.start()
    for copy in copies:
        copy.wait()


def per_device(gr, fs, tp, tokens, norm_gain, up_weight, down_weight):
    rows, width = up_weight.shape
    units, cols = down_weight.shape
    group = gr * tp
    chips = group // 2
    slices = max(1, rows // 2 // SLICE_ROWS)
    single = slices * SINGLE_NUM // SINGLE_DEN if chips > 1 else 0
    block = width * group // fs
    blocks = width // block
    count, depth = tokens.shape
    model = cols * group
    pairs = fs // 2
    wide = model // fs
    assert pairs == group and pairs > 1
    vmem = pl.BlockSpec(memory_space=pltpu.VMEM)
    hbm = pl.BlockSpec(memory_space=pltpu.HBM)
    bf16, f32 = jnp.bfloat16, jnp.float32
    dma = pltpu.SemaphoreType.DMA
    results = (
        jax.ShapeDtypeStruct((depth, block), bf16),
        jax.ShapeDtypeStruct((units, model), bf16),
        jax.ShapeDtypeStruct((count, wide), bf16),
    )
    arrays = pl.pallas_call(
        functools.partial(fused_kernel, tp, blocks, fs, single),
        out_shape=results,
        in_specs=[hbm] * 4,
        out_specs=(vmem,) * 3,
        scratch_shapes=[
            pltpu.VMEM(tokens.shape, bf16),
            pltpu.VMEM((1, rows), f32),
            pltpu.VMEM(up_weight.shape, f32),
            pltpu.VMEM(down_weight.shape, f32),
            dma((4,)),
            pltpu.VMEM((chips, rows, width), bf16),
            pltpu.VMEM((fs, count, rows), bf16),
            pltpu.VMEM((count, block), f32),
            pltpu.VMEM((count, block), bf16),
            pltpu.VMEM((fs, count, wide), bf16),
            pltpu.VMEM((pairs, count, wide), bf16),
            pltpu.VMEM((pairs, count, wide), bf16),
            pltpu.VMEM((pairs + 1, count, wide), bf16),
            *[dma((chips, blocks, 2 * slices)) for _ in range(3)], dma((2 * fs,)), dma((fs, chips)),
            dma((fs,)), dma((fs,)), dma((1,)), dma((1,)),
            *[dma((chips, 2, DOWN_CHUNKS)) for _ in range(4)],
            *[dma((pairs, PIECES)) for _ in range(3)], dma((pairs + 1, PIECES)),
        ],
        compiler_params=pltpu.CompilerParams(
            collective_id=0, has_side_effects=True, vmem_limit_bytes=FUSED_VMEM * MIB
        ),
        cost_estimate=pl.CostEstimate(
            flops=2 * count * block * (depth + model), bytes_accessed=160 * MIB, transcendentals=0
        ),
    )(*[pltpu.with_memory_space_constraint(x, pltpu.HBM) for x in (tokens, norm_gain[None, :], up_weight, down_weight)])
    return pl.pallas_call(
        copy_kernel,
        out_shape=results,
        in_specs=[vmem] * 3,
        out_specs=(hbm,) * 3,
        scratch_shapes=[dma((3, COPY_CHUNKS))],
        compiler_params=pltpu.CompilerParams(vmem_limit_bytes=COPY_VMEM * MIB),
        cost_estimate=pl.CostEstimate(flops=count * wide, bytes_accessed=18 * MIB, transcendentals=0),
    )(*arrays)


def solution(mesh):
    in_specs = (P(("gr", "tp"), None), P("fs"), P("fs", ("gr", "tp")), P("fs", ("gr", "tp")))
    out_specs = (P(None, "fs"), P("fs", None), P(("gr", "tp"), "fs"))
    body = functools.partial(per_device, mesh.shape["gr"], mesh.shape["fs"], mesh.shape["tp"])
    return jax.shard_map(
        body, mesh=mesh, in_specs=in_specs, out_specs=out_specs, check_vma=False
    )
```

```python
import functools

import jax
import jax.numpy as jnp
from jax import lax
from jax.experimental import pallas as pl
from jax.experimental.pallas import tpu as pltpu
from jax.sharding import PartitionSpec as P

MESH = pl.DeviceIdType.MESH
MIB = 1024 * 1024
FUSED_VMEM = 36
COPY_VMEM = 4
SLICE_ROWS = 32
SINGLE_NUM, SINGLE_DEN = 1, 4
PIECES = 4
DOWN_CHUNKS = 2
COPY_CHUNKS = 4
AHEAD = 2


def flipped(index, step, count):
    if count & (count - 1):
        return lax.rem(index + step, count)
    bit = 1
    while bit < count:
        if step & bit:
            index = index + (1 - 2 * lax.rem(index // bit, 2)) * bit
        bit *= 2
    return index


def remote(src, dst, send, recv, device):
    return pltpu.make_async_remote_copy(
        src_ref=src, dst_ref=dst, send_sem=send, recv_sem=recv,
        device_id=device, device_id_type=MESH,
    )


def when_not(condition):
    return pl.when(jnp.logical_not(condition))


def fused_kernel(
    tp, blocks, shards, single, tokens_in, gain_in, up_in, down_in, up_out, down_out, mixed,
    tokens, gain, up, down, loads, gath, normed, acc, hidden, part, ybuf, zout, zin,
    xs, xr, fsend, frecv, msend, ps, pr, ods, odr, xds, xdr, pds, pdr, ys, yr, zs, zr,
):
    load = [
        pltpu.make_async_copy(source, kept, loads.at[i])
        for i, (source, kept) in enumerate(
            [(gain_in, gain), (up_in, up), (down_in, down), (tokens_in, tokens)]
        )
    ]
    for copy in load:
        copy.start()
    g, f, t = lax.axis_index("gr"), lax.axis_index("fs"), lax.axis_index("tp")
    per = tp // 2
    chips = gath.shape[0]
    c, k = g * per + t // 2, lax.rem(t, 2)
    rows, width = up.shape
    half = rows // 2
    block = width // blocks
    cols = down.shape[1]
    pairs = ybuf.shape[0]
    wide = mixed.shape[1]
    z, y = f // 2, lax.rem(f, 2)

    def dev(chip, shard, core):
        return (chip // per, shard, lax.rem(chip, per) * 2 + core)

    def down_cols(pair):
        return pl.ds(pl.multiple_of(pair * cols, cols), cols)

    barrier = pltpu.get_barrier_semaphore()
    for s in range(1, chips):
        pl.semaphore_signal(
            barrier, inc=1, device_id=dev(lax.rem(c + s, chips), f, k), device_id_type=MESH
        )
    for s in range(shards):
        for core in range(2):
            if s == 0 and core == 0:
                continue
            other = lax.rem(f + s, shards)
            core_id = lax.rem(k + core, 2)
            pl.semaphore_signal(
                barrier, inc=1, device_id=dev(c, other, core_id), device_id_type=MESH
            )

    load[0].wait()
    square = (rows, rows)
    diagonal = lax.broadcasted_iota(jnp.int32, square, 0) == lax.broadcasted_iota(jnp.int32, square, 1)
    column = jnp.sum(jnp.where(diagonal, gain[...], 0.0), axis=1, keepdims=True)
    load[1].wait()
    gath[c] = (column * up[...]).astype(jnp.bfloat16)
    pl.semaphore_wait(barrier, chips - 1 + 2 * shards - 1)

    slices = xs.shape[2] // 2
    piece = half // slices

    def route(u):
        q = u % slices
        return 1 if q < single else 0 if q < 2 * single else None

    def crosses(source, target):
        return source // (shards // 2) != target // (shards // 2)

    def unit(chip, j, u):
        return gath.at[chip, pl.ds(u * piece, piece), pl.ds(j * block, block)]

    def half_rows(shard, core, first=0, count=half):
        at = pl.multiple_of(shard * rows + core * half + first, piece)
        return up_out.at[pl.ds(at, count), :]

    def target(chip, j):
        return (chip * 2 + k) * blocks + j

    def landing(u):
        return up_out.at[pl.ds(pl.multiple_of(f * rows + u * piece, piece), piece), :]

    def stays(chip, j, u):
        return jnp.logical_and(target(chip, j) == f, k == u // slices)

    def forward(chip, j, u):
        to = target(chip, j)
        at = f if route(u) is None else f + jnp.where(crosses(f, to), shards, 0)
        return remote(
            unit(chip, j, u), landing(u), fsend.at[chip, j, u], frecv.at[at], dev(c, to, u // slices)
        )

    def start_forward(chip, j, u):
        @when_not(stays(chip, j, u))
        def _():
            forward(chip, j, u).start()

        @pl.when(stays(chip, j, u))
        def _():
            landing(u)[...] = unit(chip, j, u)[...]

    def goes(chip, j, u, offset, action):
        if route(u) is None or route(u) == offset:
            action()
        else:
            when_not(crosses(f, target(chip, j)))(action)

    def exchange(s, j, u):
        return remote(
            unit(c, j, u), unit(c, j, u), xs.at[s, j, u], xr.at[s, j, u],
            dev(lax.rem(c + s, chips), f, k),
        )

    def exchanged(s, j, u):
        source = lax.rem(c + chips - s, chips)
        return remote(
            unit(source, j, u), unit(source, j, u), xs.at[s, j, u], xr.at[s, j, u], dev(c, f, k)
        )

    units = [
        [(j, q + core * slices) for core in range(2) for j in range(blocks)] for q in range(slices)
    ]
    for group in units:
        for j, u in group:
            for s in range(1, chips):
                goes(c, j, u, s, lambda: exchange(s, j, u).start())
            if route(u) in (None, 0):
                pl.when(crosses(f, target(c, j)))(lambda: forward(c, j, u).start())

    load[2].wait()
    own_pair = c * 2 + k
    down_out[:, down_cols(own_pair)] = down[...].astype(jnp.bfloat16)
    down_half = down.shape[0] // 2
    chunks = xds.shape[2]
    chunk = down_half // chunks

    def down_own(core):
        held = down_out.at[:, down_cols(c * 2 + core)]
        return remote(held, held, ods.at[0], odr.at[0], dev(c, f, 1 - k))

    down_own(k).start()

    def pair_of(chip, position):
        low = 2 * chip
        return low + jnp.where(z <= low, 1 - position, position)

    def down_piece(pair, core, i):
        at = pl.multiple_of(core * down_half + i * chunk, chunk)
        return down_out.at[pl.ds(at, chunk), down_cols(pair)]

    def down_across(s, position, i):
        held = down_piece(pair_of(c, position), k, i)
        return remote(
            held, held, xds.at[s, position, i], xdr.at[s, position, i],
            dev(lax.rem(c + s, chips), f, k),
        )

    def down_relay(s, position, i, core):
        held = down_piece(pair_of(lax.rem(c + chips - s, chips), position), core, i)
        return remote(held, held, pds.at[s, position, i], pdr.at[s, position, i], dev(c, f, 1 - k))

    def down_arrival(s, position, i):
        held = down_piece(pair_of(lax.rem(c + chips - s, chips), position), k, i)
        return remote(held, held, xds.at[s, position, i], xdr.at[s, position, i], dev(c, f, k))

    load[3].wait()
    widened = tokens[...].astype(jnp.float32)
    scale = lax.rsqrt(jnp.mean(widened * widened, axis=-1, keepdims=True) + 1e-06)
    for shard in range(shards):
        share = tokens[:, shard * rows:(shard + 1) * rows].astype(jnp.float32)
        normed[shard] = (share * scale).astype(jnp.bfloat16)

    owner = f // (2 * blocks)
    offset = lax.rem(c + chips - owner, chips)
    lone = single * piece

    def alone(shard):
        return jnp.logical_and(crosses(shard, f), offset < 2)

    def lone_rows(shard):
        return half_rows(shard, k, (1 - offset) * lone, lone)

    def lone_arrival(shard):
        return remote(
            lone_rows(shard), lone_rows(shard), msend.at[shard, 0], frecv.at[shards + shard], dev(c, f, k)
        )

    def lone_relay(shard, s):
        return remote(
            lone_rows(shard), lone_rows(shard), msend.at[shard, s], frecv.at[shard],
            dev(lax.rem(c + s, chips), f, k),
        )

    even = not shards & (shards - 1)
    far = [s for s in range(1, shards) if single and (not even or s & (shards // 2))]

    def relay_lone():
        for step in far:
            shard = flipped(f, step, shards)

            @pl.when(alone(shard))
            def _():
                lone_arrival(shard).wait_recv()
                for s in range(1, chips):
                    lone_relay(shard, s).start()

    def send_down():
        down_own(1 - k).wait_recv()
        for position in range(2):
            for i in range(chunks):
                for s in range(1, chips):
                    down_across(s, position, i).start()

    for q, group in enumerate(units):
        for j, u in group:
            when_not(crosses(f, target(c, j)))(lambda: start_forward(c, j, u))
            for s in range(1, chips):
                source = lax.rem(c + chips - s, chips)

                def pass_on():
                    exchanged(s, j, u).wait_recv()
                    start_forward(source, j, u)

                goes(source, j, u, s, pass_on)
    relay_lone()
    send_down()

    source_core = lax.rem(f // blocks, 2)
    own_stays = source_core == k

    def arrive(shard, step):
        def arrival(count):
            held = half_rows(shard, k, 0, count)
            return remote(held, held, ps.at[shard], frecv.at[shard], dev(c, f, 1 - k))

        if step in far:
            @pl.when(alone(shard))
            def _():
                arrival(half - lone).wait_recv()

            @when_not(alone(shard))
            def _():
                arrival(half).wait_recv()
        elif step == 0:
            @when_not(own_stays)
            def _():
                arrival(half).wait_recv()
        else:
            arrival(half).wait_recv()

    def relay(shard, core):
        held = half_rows(shard, core)
        return remote(held, held, ps.at[shard], pr.at[shard], dev(c, f, 1 - k))

    def accumulate(shard, first):
        weights = up_out[pl.ds(pl.multiple_of(shard * rows, rows), rows), :]
        product = jnp.dot(normed[shard], weights, preferred_element_type=jnp.float32)
        if first:
            acc[...] = product
        else:
            acc[...] += product

    near = shards // 2
    steps = list(range(1, near)) + [0] + list(range(near, shards))
    order = [flipped(f, s, shards) for s in steps]
    for position, shard in enumerate(order):
        arrive(shard, steps[position])
        relay(shard, k).start()
        if position > 0:
            before = order[position - 1]
            relay(before, 1 - k).wait_recv()
            accumulate(before, position == 1)
    relay(order[-1], 1 - k).wait_recv()
    accumulate(order[-1], False)
    hidden[...] = jnp.square(jnp.maximum(acc[...], 0.0)).astype(jnp.bfloat16)

    pieces = ys.shape[1]
    span = mixed.shape[0] // pieces

    def across(pair, i):
        at = pl.ds(i * span, span)
        return remote(
            part.at[2 * pair + 1 - y, at], ybuf.at[pair, at], ys.at[pair, i], yr.at[pair, i],
            dev(c, z * 2 + 1 - y, k),
        )

    def along(pair, i):
        at = pl.ds(i * span, span)
        to = z + jnp.where(pair > z, 1, -1)
        slot = jnp.where(jnp.logical_and(pair < z, pair == to), pairs, pair)
        return remote(
            zout.at[pair, at], zin.at[slot, at], zs.at[pair, i], zr.at[slot, i], dev(c, to * 2 + y, k)
        )

    def carried(slot, i):
        held = zin.at[slot, pl.ds(i * span, span)]
        return remote(held, held, zs.at[0, i], zr.at[slot, i], dev(c, f, k))

    def multiply(pair):
        both = jnp.dot(
            hidden[...], down_out[:, down_cols(pair)], preferred_element_type=jnp.float32
        ).astype(jnp.bfloat16)
        part[2 * pair] = both[:, :wide]
        part[2 * pair + 1] = both[:, wide:]
        for i in range(pieces):
            across(pair, i).start()

    def reduce(pair):
        inner = jnp.logical_and(pair != z, jnp.where(pair > z, z > 0, z < pairs - 1))
        outer = jnp.logical_and(pair != z, jnp.logical_not(inner))
        for i in range(pieces):
            at = pl.ds(i * span, span)

            def wide_of(ref, slot):
                return ref[slot, at].astype(jnp.float32)

            def summed():
                return wide_of(part, 2 * pair + y) + wide_of(ybuf, pair)

            across(pair, i).wait_recv()

            @pl.when(inner)
            def _():
                carried(pair, i).wait_recv()
                zout[pair, at] = (summed() + wide_of(zin, pair)).astype(jnp.bfloat16)
                along(pair, i).start()

            @pl.when(outer)
            def _():
                zout[pair, at] = summed().astype(jnp.bfloat16)
                along(pair, i).start()

            @pl.when(pair == z)
            def _():
                @pl.when(z == 0)
                def _():
                    carried(pairs, i).wait_recv()
                    mixed[at] = (summed() + wide_of(zin, pairs)).astype(jnp.bfloat16)

                @pl.when(z == pairs - 1)
                def _():
                    carried(pair, i).wait_recv()
                    mixed[at] = (summed() + wide_of(zin, pair)).astype(jnp.bfloat16)

                @pl.when(jnp.logical_and(z > 0, z < pairs - 1))
                def _():
                    carried(pair, i).wait_recv()
                    carried(pairs, i).wait_recv()
                    total = summed() + wide_of(zin, pair) + wide_of(zin, pairs)
                    mixed[at] = total.astype(jnp.bfloat16)

    def fetch(s, position):
        for i in range(chunks):
            down_arrival(s, position, i).wait_recv()
            down_relay(s, position, i, k).start()
        for i in range(chunks):
            down_relay(s, position, i, 1 - k).wait_recv()

    def pair_at(index):
        return pair_of(lax.rem(c + chips - index // 2, chips), lax.rem(index, 2))

    last = 2 * lax.rem(z // 2 + chips - c, chips) + 1
    sequence = [pair_at(i + jnp.where(i < last, 0, 1)) for i in range(pairs - 1)] + [pair_at(last)]
    for i in range(pairs):
        if i > 1:
            fetch(i // 2, i % 2)
        multiply(pair_at(i))
        if i >= AHEAD:
            reduce(sequence[i - AHEAD])
    for pair in sequence[pairs - AHEAD:]:
        reduce(pair)

    down_own(k).wait_send()
    for s in range(1, chips):
        for position in range(2):
            for i in range(chunks):
                down_across(s, position, i).wait_send()
                down_relay(s, position, i, k).wait_send()
    for step in far:
        shard = flipped(f, step, shards)

        @pl.when(alone(shard))
        def _():
            for s in range(1, chips):
                lone_relay(shard, s).wait_send()
    for group in units:
        for j, u in group:
            for s in range(1, chips):
                goes(c, j, u, s, lambda: exchange(s, j, u).wait_send())
            for s in range(chips):
                source = lax.rem(c + chips - s, chips)

                def sent():
                    @when_not(stays(source, j, u))
                    def _():
                        forward(source, j, u).wait_send()

                goes(source, j, u, s, sent)
    for shard in order:
        relay(shard, k).wait_send()
    for pair in sequence:
        for i in range(pieces):
            across(pair, i).wait_send()

            @pl.when(pair != z)
            def _():
                along(pair, i).wait_send()


def copy_kernel(up, down, mixed, up_out, down_out, mixed_out, sems):
    copies = []
    for index, (source, kept) in enumerate([(up, up_out), (down, down_out), (mixed, mixed_out)]):
        count = sems.shape[1]
        span = source.shape[0] // count
        for i in range(count):
            at = pl.ds(i * span, span)
            copies.append(pltpu.make_async_copy(source.at[at], kept.at[at], sems.at[index, i]))
    for copy in copies:
        copy.start()
    for copy in copies:
        copy.wait()


def per_device(gr, fs, tp, tokens, norm_gain, up_weight, down_weight):
    rows, width = up_weight.shape
    units, cols = down_weight.shape
    group = gr * tp
    chips = group // 2
    slices = max(1, rows // 2 // SLICE_ROWS)
    single = slices * SINGLE_NUM // SINGLE_DEN if chips > 1 else 0
    block = width * group // fs
    blocks = width // block
    count, depth = tokens.shape
    model = cols * group
    pairs = fs // 2
    wide = model // fs
    assert pairs == group and pairs > 1
    vmem = pl.BlockSpec(memory_space=pltpu.VMEM)
    hbm = pl.BlockSpec(memory_space=pltpu.HBM)
    bf16, f32 = jnp.bfloat16, jnp.float32
    dma = pltpu.SemaphoreType.DMA
    results = (
        jax.ShapeDtypeStruct((depth, block), bf16),
        jax.ShapeDtypeStruct((units, model), bf16),
        jax.ShapeDtypeStruct((count, wide), bf16),
    )
    arrays = pl.pallas_call(
        functools.partial(fused_kernel, tp, blocks, fs, single),
        out_shape=results,
        in_specs=[hbm] * 4,
        out_specs=(vmem,) * 3,
        scratch_shapes=[
            pltpu.VMEM(tokens.shape, bf16),
            pltpu.VMEM((1, rows), f32),
            pltpu.VMEM(up_weight.shape, f32),
            pltpu.VMEM(down_weight.shape, f32),
            dma((4,)),
            pltpu.VMEM((chips, rows, width), bf16),
            pltpu.VMEM((fs, count, rows), bf16),
            pltpu.VMEM((count, block), f32),
            pltpu.VMEM((count, block), bf16),
            pltpu.VMEM((fs, count, wide), bf16),
            pltpu.VMEM((pairs, count, wide), bf16),
            pltpu.VMEM((pairs, count, wide), bf16),
            pltpu.VMEM((pairs + 1, count, wide), bf16),
            *[dma((chips, blocks, 2 * slices)) for _ in range(3)], dma((2 * fs,)), dma((fs, chips)),
            dma((fs,)), dma((fs,)), dma((1,)), dma((1,)),
            *[dma((chips, 2, DOWN_CHUNKS)) for _ in range(4)],
            *[dma((pairs, PIECES)) for _ in range(3)], dma((pairs + 1, PIECES)),
        ],
        compiler_params=pltpu.CompilerParams(
            collective_id=0, has_side_effects=True, vmem_limit_bytes=FUSED_VMEM * MIB
        ),
        cost_estimate=pl.CostEstimate(
            flops=2 * count * block * (depth + model), bytes_accessed=160 * MIB, transcendentals=0
        ),
    )(*[pltpu.with_memory_space_constraint(x, pltpu.HBM) for x in (tokens, norm_gain[None, :], up_weight, down_weight)])
    return pl.pallas_call(
        copy_kernel,
        out_shape=results,
        in_specs=[vmem] * 3,
        out_specs=(hbm,) * 3,
        scratch_shapes=[dma((3, COPY_CHUNKS))],
        compiler_params=pltpu.CompilerParams(vmem_limit_bytes=COPY_VMEM * MIB),
        cost_estimate=pl.CostEstimate(flops=count * wide, bytes_accessed=18 * MIB, transcendentals=0),
    )(*arrays)


def solution(mesh):
    in_specs = (P(("gr", "tp"), None), P("fs"), P("fs", ("gr", "tp")), P("fs", ("gr", "tp")))
    out_specs = (P(None, "fs"), P("fs", None), P(("gr", "tp"), "fs"))
    body = functools.partial(per_device, mesh.shape["gr"], mesh.shape["fs"], mesh.shape["tp"])
    return jax.shard_map(
        body, mesh=mesh, in_specs=in_specs, out_specs=out_specs, check_vma=False
    )
```

```python
import functools

import jax
import jax.numpy as jnp
from jax import lax
from jax.experimental import pallas as pl
from jax.experimental.pallas import tpu as pltpu
from jax.sharding import PartitionSpec as P

MESH = pl.DeviceIdType.MESH
MIB = 1024 * 1024
FUSED_VMEM = 36
COPY_VMEM = 4
SLICE_ROWS = 32
SINGLE = ((1, 4), (1, 4))
PIECES = 4
DOWN_CHUNKS = 2
COPY_CHUNKS = 2


def flipped(index, step, count):
    if count & (count - 1):
        return lax.rem(index + step, count)
    bit = 1
    while bit < count:
        if step & bit:
            index = index + (1 - 2 * lax.rem(index // bit, 2)) * bit
        bit *= 2
    return index


def remote(src, dst, send, recv, device):
    return pltpu.make_async_remote_copy(
        src_ref=src, dst_ref=dst, send_sem=send, recv_sem=recv,
        device_id=device, device_id_type=MESH,
    )


def when_not(condition):
    return pl.when(jnp.logical_not(condition))


def fused_kernel(
    tp, blocks, shards, single, tokens_in, gain_in, up_in, down_in, up_out, down_out, mixed,
    tokens, gain, up, down, loads, gath, normed, acc, hidden, part, ybuf, zout, zin,
    xs, xr, fsend, frecv, msend, ps, pr, ods, odr, xds, xdr, pds, pdr, ys, yr, zs, zr,
):
    load = [
        pltpu.make_async_copy(source, kept, loads.at[i])
        for i, (source, kept) in enumerate(
            [(gain_in, gain), (up_in, up), (down_in, down), (tokens_in, tokens)]
        )
    ]
    for copy in load:
        copy.start()
    g, f, t = lax.axis_index("gr"), lax.axis_index("fs"), lax.axis_index("tp")
    per = tp // 2
    chips = gath.shape[0]
    c, k = g * per + t // 2, lax.rem(t, 2)
    rows, width = up.shape
    half = rows // 2
    block = width // blocks
    cols = down.shape[1]
    pairs = ybuf.shape[0]
    wide = mixed.shape[1]
    z, y = f // 2, lax.rem(f, 2)

    def dev(chip, shard, core):
        return (chip // per, shard, lax.rem(chip, per) * 2 + core)

    def down_cols(pair):
        return pl.ds(pl.multiple_of(pair * cols, cols), cols)

    barrier = pltpu.get_barrier_semaphore()
    for s in range(1, chips):
        pl.semaphore_signal(
            barrier, inc=1, device_id=dev(lax.rem(c + s, chips), f, k), device_id_type=MESH
        )
    for s in range(shards):
        for core in range(2):
            if s == 0 and core == 0:
                continue
            other = lax.rem(f + s, shards)
            core_id = lax.rem(k + core, 2)
            pl.semaphore_signal(
                barrier, inc=1, device_id=dev(c, other, core_id), device_id_type=MESH
            )

    load[0].wait()
    square = (rows, rows)
    diagonal = lax.broadcasted_iota(jnp.int32, square, 0) == lax.broadcasted_iota(jnp.int32, square, 1)
    column = jnp.sum(jnp.where(diagonal, gain[...], 0.0), axis=1, keepdims=True)
    load[1].wait()
    gath[c] = (column * up[...]).astype(jnp.bfloat16)
    pl.semaphore_wait(barrier, chips - 1 + 2 * shards - 1)

    slices = xr.shape[2] // 2
    piece = half // slices

    def route(u):
        q = u % slices
        return 1 if q < single[1] else 0 if q < sum(single) else None

    def crosses(source, target):
        return source // (shards // 2) != target // (shards // 2)

    def unit(chip, j, u):
        return gath.at[chip, pl.ds(u * piece, piece), pl.ds(j * block, block)]

    def half_rows(shard, core, first=0, count=half):
        at = pl.multiple_of(shard * rows + core * half + first, piece)
        return up_out.at[pl.ds(at, count), :]

    def target(chip, j):
        return (chip * 2 + k) * blocks + j

    def landing(u):
        return up_out.at[pl.ds(pl.multiple_of(f * rows + u * piece, piece), piece), :]

    def stays(chip, j, u):
        return jnp.logical_and(target(chip, j) == f, k == u // slices)

    def pinned(u, s):
        return 0 if route(u) in (None, s) else 1

    def forward(chip, j, u, s):
        to = target(chip, j)
        at = f if route(u) is None else f + jnp.where(crosses(f, to), shards, 0)
        return remote(
            unit(chip, j, u), landing(u), fsend.at[s, j, pinned(u, s)], frecv.at[at],
            dev(c, to, u // slices),
        )

    def start_forward(chip, j, u, s):
        @when_not(stays(chip, j, u))
        def _():
            forward(chip, j, u, s).start()

        @pl.when(stays(chip, j, u))
        def _():
            landing(u)[...] = unit(chip, j, u)[...]

    def goes(chip, j, u, offset, action):
        if route(u) is None or route(u) == offset:
            action()
        else:
            when_not(crosses(f, target(chip, j)))(action)

    def exchange(s, j, u):
        return remote(
            unit(c, j, u), unit(c, j, u), xs.at[s - 1, pinned(u, s)], xr.at[s - 1, j, u],
            dev(lax.rem(c + s, chips), f, k),
        )

    def exchanged(s, j, u):
        source = lax.rem(c + chips - s, chips)
        return remote(
            unit(source, j, u), unit(source, j, u), xs.at[s - 1, 0], xr.at[s - 1, j, u], dev(c, f, k)
        )

    units = [
        [(j, q + core * slices) for core in range(2) for j in range(blocks)] for q in range(slices)
    ]
    for group in units:
        for j, u in group:
            for s in range(1, chips):
                goes(c, j, u, s, lambda: exchange(s, j, u).start())
            if route(u) in (None, 0):
                pl.when(crosses(f, target(c, j)))(lambda: forward(c, j, u, 0).start())

    load[2].wait()
    own_pair = c * 2 + k
    down_out[:, down_cols(own_pair)] = down[...].astype(jnp.bfloat16)
    down_half = down.shape[0] // 2
    chunks = xdr.shape[2]
    chunk = down_half // chunks

    def down_own(core):
        held = down_out.at[:, down_cols(c * 2 + core)]
        return remote(held, held, ods.at[0], odr.at[0], dev(c, f, 1 - k))

    down_own(k).start()

    def pair_of(chip, position):
        low = 2 * chip
        return low + jnp.where(z <= low, 1 - position, position)

    def down_piece(pair, core, i):
        at = pl.multiple_of(core * down_half + i * chunk, chunk)
        return down_out.at[pl.ds(at, chunk), down_cols(pair)]

    def down_across(s, position, i):
        held = down_piece(pair_of(c, position), k, i)
        return remote(
            held, held, xds.at[0], xdr.at[s - 1, position, i], dev(lax.rem(c + s, chips), f, k)
        )

    def down_relay(s, position, i):
        held = down_piece(pair_of(lax.rem(c + chips - s, chips), position), k, i)
        return remote(held, held, pds.at[0], pdr.at[s - 1, position, i], dev(c, f, 1 - k))

    def down_arrival(s, position, i, semaphore):
        held = down_piece(0, k, i)
        return remote(held, held, xds.at[0], semaphore.at[s - 1, position, i], dev(c, f, k))

    load[3].wait()
    widened = tokens[...].astype(jnp.float32)
    scale = lax.rsqrt(jnp.mean(widened * widened, axis=-1, keepdims=True) + 1e-06)
    for shard in range(shards):
        share = tokens[:, shard * rows:(shard + 1) * rows].astype(jnp.float32)
        normed[shard] = (share * scale).astype(jnp.bfloat16)

    owner = f // (2 * blocks)
    offset = lax.rem(c + chips - owner, chips)
    lone = [count * piece for count in single]

    def alone(shard, way):
        return jnp.logical_and(crosses(shard, f), offset == way)

    def lone_rows(shard, way):
        return half_rows(shard, k, lone[1] if way == 0 else 0, lone[way])

    def lone_arrival(shard, way):
        held = lone_rows(shard, way)
        return remote(held, held, msend.at[0], frecv.at[shards + shard], dev(c, f, k))

    def lone_relay(shard, way, s):
        held = lone_rows(shard, way)
        return remote(
            held, held, msend.at[0], frecv.at[shard], dev(lax.rem(c + s, chips), f, k)
        )

    ways = [way for way in range(2) if single[way]]
    even = not shards & (shards - 1)
    far = [s for s in range(1, shards) if sum(single) and (not even or s & (shards // 2))]

    def relay_lone():
        for step in far:
            shard = flipped(f, step, shards)

            for way in ways:
                @pl.when(alone(shard, way))
                def _():
                    lone_arrival(shard, way).wait_recv()
                    for s in range(1, chips):
                        lone_relay(shard, way, s).start()

    order_down = [(position, i) for position in range(2) for i in range(chunks)]

    def send_down(pieces_of):
        for position, i in pieces_of:
            for s in range(1, chips):
                down_across(s, position, i).start()

    early = crosses(f, target(c, 0))

    @pl.when(early)
    def _():
        down_own(1 - k).wait_recv()
        send_down(order_down[:1])

    for q, group in enumerate(units):
        if q == max(0, slices - 1):
            @pl.when(early)
            def _():
                relay_lone()
                send_down(order_down[1:])

        for j, u in group:
            when_not(crosses(f, target(c, j)))(lambda: start_forward(c, j, u, 0))
            for s in range(1, chips):
                source = lax.rem(c + chips - s, chips)

                def pass_on():
                    exchanged(s, j, u).wait_recv()
                    start_forward(source, j, u, s)

                goes(source, j, u, s, pass_on)

    @when_not(early)
    def _():
        relay_lone()
        down_own(1 - k).wait_recv()
        send_down(order_down)

    source_core = lax.rem(f // blocks, 2)
    own_stays = source_core == k

    def arrive(shard, step):
        def arrival(count):
            held = half_rows(shard, k, 0, count)
            return remote(held, held, ps.at[0], frecv.at[shard], dev(c, f, 1 - k))

        if step in far:
            whole = jnp.logical_not(crosses(shard, f))
            for way in ways:
                pl.when(alone(shard, way))(lambda: arrival(half - lone[way]).wait_recv())
            rest = jnp.logical_or(whole, functools.reduce(jnp.logical_and, [offset != way for way in ways]))
            pl.when(rest)(lambda: arrival(half).wait_recv())
        elif step == 0:
            @when_not(own_stays)
            def _():
                arrival(half).wait_recv()
        else:
            arrival(half).wait_recv()

    def relay(shard, core):
        held = half_rows(shard, core)
        return remote(held, held, ps.at[0], pr.at[shard], dev(c, f, 1 - k))

    def accumulate(shard, first):
        weights = up_out[pl.ds(pl.multiple_of(shard * rows, rows), rows), :]
        product = jnp.dot(normed[shard], weights, preferred_element_type=jnp.float32)
        if first:
            acc[...] = product
        else:
            acc[...] += product

    near = shards // 2
    steps = list(range(1, near)) + [0] + list(range(near, shards))
    order = [flipped(f, s, shards) for s in steps]
    for position, shard in enumerate(order):
        arrive(shard, steps[position])
        relay(shard, k).start()
        if position > 0:
            before = order[position - 1]
            relay(before, 1 - k).wait_recv()
            accumulate(before, position == 1)
    relay(order[-1], 1 - k).wait_recv()
    accumulate(order[-1], False)
    hidden[...] = jnp.square(jnp.maximum(acc[...], 0.0)).astype(jnp.bfloat16)

    pieces = yr.shape[1]
    span = mixed.shape[0] // pieces

    def place(i):
        return pl.ds(i * span, span)

    def across(pair, i):
        at = place(i)
        return remote(
            part.at[2 * pair + 1 - y, at], ybuf.at[pair, at], ys.at[0], yr.at[pair, i],
            dev(c, z * 2 + 1 - y, k),
        )

    def along(pair, i):
        at = place(i)
        to = z + jnp.where(pair > z, 1, -1)
        slot = jnp.where(jnp.logical_and(pair < z, pair == to), pairs, pair)
        return remote(
            zout.at[pair, at], zin.at[slot, at], zs.at[0], zr.at[slot, i], dev(c, to * 2 + y, k)
        )

    def carried(slot, i):
        held = zin.at[slot, place(i)]
        return remote(held, held, zs.at[0], zr.at[slot, i], dev(c, f, k))

    def multiply(pair):
        both = jnp.dot(
            hidden[...], down_out[:, down_cols(pair)], preferred_element_type=jnp.float32
        ).astype(jnp.bfloat16)
        part[2 * pair] = both[:, :wide]
        part[2 * pair + 1] = both[:, wide:]
        for i in range(pieces):
            across(pair, i).start()

    def reduce(pair):
        inner = jnp.logical_and(pair != z, jnp.where(pair > z, z > 0, z < pairs - 1))
        outer = jnp.logical_and(pair != z, jnp.logical_not(inner))
        for i in range(pieces):
            at = place(i)

            def wide_of(ref, slot):
                return ref[slot, at].astype(jnp.float32)

            def summed():
                return wide_of(part, 2 * pair + y) + wide_of(ybuf, pair)

            across(pair, i).wait_recv()

            @pl.when(inner)
            def _():
                carried(pair, i).wait_recv()
                zout[pair, at] = (summed() + wide_of(zin, pair)).astype(jnp.bfloat16)
                along(pair, i).start()

            @pl.when(outer)
            def _():
                zout[pair, at] = summed().astype(jnp.bfloat16)
                along(pair, i).start()

            @pl.when(pair == z)
            def _():
                @pl.when(z == 0)
                def _():
                    carried(pairs, i).wait_recv()
                    mixed[at] = (summed() + wide_of(zin, pairs)).astype(jnp.bfloat16)

                @pl.when(z == pairs - 1)
                def _():
                    carried(pair, i).wait_recv()
                    mixed[at] = (summed() + wide_of(zin, pair)).astype(jnp.bfloat16)

                @pl.when(jnp.logical_and(z > 0, z < pairs - 1))
                def _():
                    carried(pair, i).wait_recv()
                    carried(pairs, i).wait_recv()
                    total = summed() + wide_of(zin, pair) + wide_of(zin, pairs)
                    mixed[at] = total.astype(jnp.bfloat16)

    def fetch(s, position):
        for i in range(chunks):
            down_arrival(s, position, i, xdr).wait_recv()
            down_relay(s, position, i).start()
        for i in range(chunks):
            down_arrival(s, position, i, pdr).wait_recv()

    def pair_at(index):
        return pair_of(lax.rem(c + chips - index // 2, chips), lax.rem(index, 2))

    last = 2 * lax.rem(z // 2 + chips - c, chips) + 1
    home = last == 1

    def index_at(i):
        return last if i == pairs - 1 else i + jnp.where(i < last, 0, 1)

    sequence = [pair_at(index_at(i)) for i in range(pairs)]

    def take(i):
        if i > 0:
            index = index_at(i)
            pl.when(index > 1)(lambda: fetch(index // 2, lax.rem(index, 2)))
        multiply(sequence[i])

    def sent(source, semaphore):
        remote(source, source, semaphore, xr.at[0, 0, 0], dev(c, f, k)).wait_send()

    def gathered():
        down_own(k).wait_send()
        for way in ways:
            passed = (chips - 1) * (shards // 2) * lone[way]
            pl.when(offset == way)(lambda: sent(up_out.at[pl.ds(0, passed), :], msend.at[0]))
        sent(up_out.at[pl.ds(0, shards * half), :], ps.at[0])
        for s in range(chips):
            source = lax.rem(c + chips - s, chips)
            count = [piece * sum(pinned(u, s) == which for u in range(2 * slices)) for which in range(2)]
            for which in range(2):
                if not count[which]:
                    continue
                if s > 0:
                    def crossed():
                        sent(gath.at[0, pl.ds(0, count[which]), :], xs.at[s - 1, which])

                    if which:
                        when_not(crosses(f, target(c, 0)))(crossed)
                    else:
                        crossed()
                for j in range(blocks):
                    to = target(source, j)

                    def left(rows_left):
                        sent(gath.at[0, pl.ds(0, rows_left), pl.ds(0, block)], fsend.at[s, j, which])

                    gone = jnp.logical_not(crosses(f, to)) if which else to >= 0
                    pl.when(jnp.logical_and(gone, to != f))(lambda: left(count[which]))
                    pl.when(to == f)(lambda: left(count[which] // 2))

    def run(*events):
        for action, i in events:
            (take if action == "take" else settle)(i)

    def settle(i):
        reduce(sequence[i])

    outer = jnp.logical_or(z == 0, z == pairs - 1)
    own = pairs - 1
    takes = [("take", i) for i in range(2, own)]
    take(0)
    take(1)
    gathered()

    @pl.when(jnp.logical_and(home, outer))
    def _():
        run(("settle", 0), *takes, ("take", own))

    @pl.when(jnp.logical_and(home, jnp.logical_not(outer)))
    def _():
        run(*takes, ("take", own), ("settle", 0))

    @when_not(home)
    def _():
        run(*takes, ("settle", 0))

        @pl.when(outer)
        def _():
            settle(1)

        take(own)

        @when_not(outer)
        def _():
            settle(1)

    @pl.when(home)
    def _():
        settle(1)

    for i in range(2, pairs):
        settle(i)

    crossed = down_out.at[pl.ds(0, down_half), pl.ds(0, 2 * (chips - 1) * cols)]
    sent(crossed, xds.at[0])
    sent(crossed, pds.at[0])
    sent(part.at[pl.ds(0, pairs)], ys.at[0])
    sent(zout.at[pl.ds(0, pairs - 1)], zs.at[0])


def copy_kernel(up, down, mixed, up_out, down_out, mixed_out, sems):
    copies = []
    for index, (source, kept) in enumerate([(up, up_out), (down, down_out), (mixed, mixed_out)]):
        count = sems.shape[1]
        span = source.shape[0] // count
        for i in range(count):
            at = pl.ds(i * span, span)
            copies.append(pltpu.make_async_copy(source.at[at], kept.at[at], sems.at[index, i]))
    for copy in copies:
        copy.start()
    for copy in copies:
        copy.wait()


def per_device(gr, fs, tp, tokens, norm_gain, up_weight, down_weight):
    rows, width = up_weight.shape
    units, cols = down_weight.shape
    group = gr * tp
    chips = group // 2
    slices = max(1, rows // 2 // SLICE_ROWS)
    single = [slices * some // of if chips > 1 else 0 for some, of in SINGLE]
    block = width * group // fs
    blocks = width // block
    count, depth = tokens.shape
    model = cols * group
    pairs = fs // 2
    wide = model // fs
    assert pairs == group and pairs > 2 and pairs % blocks == 0
    others = max(1, chips - 1)
    vmem = pl.BlockSpec(memory_space=pltpu.VMEM)
    hbm = pl.BlockSpec(memory_space=pltpu.HBM)
    bf16, f32 = jnp.bfloat16, jnp.float32
    dma = pltpu.SemaphoreType.DMA
    results = (
        jax.ShapeDtypeStruct((depth, block), bf16),
        jax.ShapeDtypeStruct((units, model), bf16),
        jax.ShapeDtypeStruct((count, wide), bf16),
    )
    arrays = pl.pallas_call(
        functools.partial(fused_kernel, tp, blocks, fs, single),
        out_shape=results,
        in_specs=[hbm] * 4,
        out_specs=(vmem,) * 3,
        scratch_shapes=[
            pltpu.VMEM(tokens.shape, bf16),
            pltpu.VMEM((1, rows), f32),
            pltpu.VMEM(up_weight.shape, f32),
            pltpu.VMEM(down_weight.shape, f32),
            dma((4,)),
            pltpu.VMEM((chips, rows, width), bf16),
            pltpu.VMEM((fs, count, rows), bf16),
            pltpu.VMEM((count, block), f32),
            pltpu.VMEM((count, block), bf16),
            pltpu.VMEM((fs, count, wide), bf16),
            pltpu.VMEM((pairs, count, wide), bf16),
            pltpu.VMEM((pairs, count, wide), bf16),
            pltpu.VMEM((pairs + 1, count, wide), bf16),
            dma((others, 2)), dma((others, blocks, 2 * slices)), dma((chips, blocks, 2)), dma((2 * fs,)),
            dma((1,)), dma((1,)), dma((fs,)), dma((1,)), dma((1,)),
            dma((1,)), dma((others, 2, DOWN_CHUNKS)), dma((1,)), dma((others, 2, DOWN_CHUNKS)),
            dma((1,)), dma((pairs, PIECES)), dma((1,)), dma((pairs + 1, PIECES)),
        ],
        compiler_params=pltpu.CompilerParams(
            collective_id=0, has_side_effects=True, vmem_limit_bytes=FUSED_VMEM * MIB
        ),
        cost_estimate=pl.CostEstimate(
            flops=2 * count * block * (depth + model), bytes_accessed=160 * MIB, transcendentals=0
        ),
    )(*[pltpu.with_memory_space_constraint(x, pltpu.HBM) for x in (tokens, norm_gain[None, :], up_weight, down_weight)])
    return pl.pallas_call(
        copy_kernel,
        out_shape=results,
        in_specs=[vmem] * 3,
        out_specs=(hbm,) * 3,
        scratch_shapes=[dma((3, COPY_CHUNKS))],
        compiler_params=pltpu.CompilerParams(vmem_limit_bytes=COPY_VMEM * MIB),
        cost_estimate=pl.CostEstimate(flops=count * wide, bytes_accessed=18 * MIB, transcendentals=0),
    )(*arrays)


def solution(mesh):
    in_specs = (P(("gr", "tp"), None), P("fs"), P("fs", ("gr", "tp")), P("fs", ("gr", "tp")))
    out_specs = (P(None, "fs"), P("fs", None), P(("gr", "tp"), "fs"))
    body = functools.partial(per_device, mesh.shape["gr"], mesh.shape["fs"], mesh.shape["tp"])
    return jax.shard_map(
        body, mesh=mesh, in_specs=in_specs, out_specs=out_specs, check_vma=False
    )
```

```python
import functools

import jax
import jax.numpy as jnp
from jax import lax
from jax.experimental import pallas as pl
from jax.experimental.pallas import tpu as pltpu
from jax.sharding import PartitionSpec as P

MESH = pl.DeviceIdType.MESH
MIB = 1024 * 1024
FUSED_VMEM = 36
COPY_VMEM = 4
SLICE_ROWS = 32
SINGLE = ((1, 4), (1, 4))
PIECES = 4
DOWN_CHUNKS = 2
COPY_CHUNKS = 2
EARLY_SUMS = (1, 2)
LATE_SUMS = 3


def flipped(index, step, count):
    if count & (count - 1):
        return lax.rem(index + step, count)
    bit = 1
    while bit < count:
        if step & bit:
            index = index + (1 - 2 * lax.rem(index // bit, 2)) * bit
        bit *= 2
    return index


def remote(src, dst, send, recv, device):
    return pltpu.make_async_remote_copy(
        src_ref=src, dst_ref=dst, send_sem=send, recv_sem=recv,
        device_id=device, device_id_type=MESH,
    )


def when_not(condition):
    return pl.when(jnp.logical_not(condition))


def fused_kernel(
    tp, blocks, shards, single, tokens_in, gain_in, up_in, down_in, up_out, down_out, mixed,
    tokens, gain, up, down, loads, gath, normed, acc, hidden, part, ybuf, zout, zin,
    xs, xr, fsend, frecv, msend, ps, pr, ods, odr, xds, xdr, pds, pdr, ys, yr, zs, zr,
):
    load = [
        pltpu.make_async_copy(source, kept, loads.at[i])
        for i, (source, kept) in enumerate(
            [(gain_in, gain), (up_in, up), (down_in, down), (tokens_in, tokens)]
        )
    ]
    for copy in load:
        copy.start()
    g, f, t = lax.axis_index("gr"), lax.axis_index("fs"), lax.axis_index("tp")
    per = tp // 2
    chips = gath.shape[0]
    c, k = g * per + t // 2, lax.rem(t, 2)
    rows, width = up.shape
    half = rows // 2
    block = width // blocks
    cols = down.shape[1]
    pairs = ybuf.shape[0]
    wide = mixed.shape[1]
    z, y = f // 2, lax.rem(f, 2)

    def dev(chip, shard, core):
        return (chip // per, shard, lax.rem(chip, per) * 2 + core)

    def down_cols(pair):
        return pl.ds(pl.multiple_of(pair * cols, cols), cols)

    barrier = pltpu.get_barrier_semaphore()
    for s in range(1, chips):
        pl.semaphore_signal(
            barrier, inc=1, device_id=dev(lax.rem(c + s, chips), f, k), device_id_type=MESH
        )
    for s in range(shards):
        for core in range(2):
            if s == 0 and core == 0:
                continue
            other = lax.rem(f + s, shards)
            core_id = lax.rem(k + core, 2)
            pl.semaphore_signal(
                barrier, inc=1, device_id=dev(c, other, core_id), device_id_type=MESH
            )

    load[0].wait()
    square = (rows, rows)
    diagonal = lax.broadcasted_iota(jnp.int32, square, 0) == lax.broadcasted_iota(jnp.int32, square, 1)
    column = jnp.sum(jnp.where(diagonal, gain[...], 0.0), axis=1, keepdims=True)
    load[1].wait()
    gath[c] = (column * up[...]).astype(jnp.bfloat16)
    pl.semaphore_wait(barrier, chips - 1 + 2 * shards - 1)

    slices = xr.shape[2] // 2
    piece = half // slices

    def route(u):
        q = u % slices
        return 1 if q < single[1] else 0 if q < sum(single) else None

    def crosses(source, target):
        return source // (shards // 2) != target // (shards // 2)

    def unit(chip, j, u):
        return gath.at[chip, pl.ds(u * piece, piece), pl.ds(j * block, block)]

    def half_rows(shard, core, first=0, count=half):
        at = pl.multiple_of(shard * rows + core * half + first, piece)
        return up_out.at[pl.ds(at, count), :]

    def target(chip, j):
        return (chip * 2 + k) * blocks + j

    def landing(u):
        return up_out.at[pl.ds(pl.multiple_of(f * rows + u * piece, piece), piece), :]

    def stays(chip, j, u):
        return jnp.logical_and(target(chip, j) == f, k == u // slices)

    def pinned(u, s):
        return 0 if route(u) in (None, s) else 1

    def forward(chip, j, u, s):
        to = target(chip, j)
        at = f if route(u) is None else f + jnp.where(crosses(f, to), shards, 0)
        return remote(
            unit(chip, j, u), landing(u), fsend.at[s, j, pinned(u, s)], frecv.at[at],
            dev(c, to, u // slices),
        )

    def start_forward(chip, j, u, s):
        @when_not(stays(chip, j, u))
        def _():
            forward(chip, j, u, s).start()

        @pl.when(stays(chip, j, u))
        def _():
            landing(u)[...] = unit(chip, j, u)[...]

    def goes(chip, j, u, offset, action):
        if route(u) is None or route(u) == offset:
            action()
        else:
            when_not(crosses(f, target(chip, j)))(action)

    def exchange(s, j, u):
        return remote(
            unit(c, j, u), unit(c, j, u), xs.at[s - 1, pinned(u, s)], xr.at[s - 1, j, u],
            dev(lax.rem(c + s, chips), f, k),
        )

    def exchanged(s, j, u):
        source = lax.rem(c + chips - s, chips)
        return remote(
            unit(source, j, u), unit(source, j, u), xs.at[s - 1, 0], xr.at[s - 1, j, u], dev(c, f, k)
        )

    units = [
        [(j, q + core * slices) for core in range(2) for j in range(blocks)] for q in range(slices)
    ]
    for group in units:
        for j, u in group:
            for s in range(1, chips):
                goes(c, j, u, s, lambda: exchange(s, j, u).start())
            if route(u) in (None, 0):
                pl.when(crosses(f, target(c, j)))(lambda: forward(c, j, u, 0).start())

    load[2].wait()
    own_pair = c * 2 + k
    down_out[:, down_cols(own_pair)] = down[...].astype(jnp.bfloat16)
    down_half = down.shape[0] // 2
    chunks = xdr.shape[2]
    chunk = down_half // chunks

    def down_own(core):
        held = down_out.at[:, down_cols(c * 2 + core)]
        return remote(held, held, ods.at[0], odr.at[0], dev(c, f, 1 - k))

    down_own(k).start()

    def pair_of(chip, position):
        low = 2 * chip
        return low + jnp.where(z <= low, 1 - position, position)

    def down_piece(pair, core, i):
        at = pl.multiple_of(core * down_half + i * chunk, chunk)
        return down_out.at[pl.ds(at, chunk), down_cols(pair)]

    def down_across(s, position, i):
        held = down_piece(pair_of(c, position), k, i)
        return remote(
            held, held, xds.at[0], xdr.at[s - 1, position, i], dev(lax.rem(c + s, chips), f, k)
        )

    def down_relay(s, position, i):
        held = down_piece(pair_of(lax.rem(c + chips - s, chips), position), k, i)
        return remote(held, held, pds.at[0], pdr.at[s - 1, position, i], dev(c, f, 1 - k))

    def down_arrival(s, position, i, semaphore):
        held = down_piece(0, k, i)
        return remote(held, held, xds.at[0], semaphore.at[s - 1, position, i], dev(c, f, k))

    load[3].wait()
    widened = tokens[...].astype(jnp.float32)
    scale = lax.rsqrt(jnp.mean(widened * widened, axis=-1, keepdims=True) + 1e-06)
    for shard in range(shards):
        share = tokens[:, shard * rows:(shard + 1) * rows].astype(jnp.float32)
        normed[shard] = (share * scale).astype(jnp.bfloat16)

    owner = f // (2 * blocks)
    offset = lax.rem(c + chips - owner, chips)
    lone = [count * piece for count in single]

    def alone(shard, way):
        return jnp.logical_and(crosses(shard, f), offset == way)

    def lone_rows(shard, way):
        return half_rows(shard, k, lone[1] if way == 0 else 0, lone[way])

    def lone_arrival(shard, way):
        held = lone_rows(shard, way)
        return remote(held, held, msend.at[0], frecv.at[shards + shard], dev(c, f, k))

    def lone_relay(shard, way, s):
        held = lone_rows(shard, way)
        return remote(
            held, held, msend.at[0], frecv.at[shard], dev(lax.rem(c + s, chips), f, k)
        )

    ways = [way for way in range(2) if single[way]]
    even = not shards & (shards - 1)
    far = [s for s in range(1, shards) if sum(single) and (not even or s & (shards // 2))]

    def relay_lone():
        for step in far:
            shard = flipped(f, step, shards)

            for way in ways:
                @pl.when(alone(shard, way))
                def _():
                    lone_arrival(shard, way).wait_recv()
                    for s in range(1, chips):
                        lone_relay(shard, way, s).start()

    order_down = [(position, i) for position in range(2) for i in range(chunks)]

    def send_down(pieces_of):
        for position, i in pieces_of:
            for s in range(1, chips):
                down_across(s, position, i).start()

    early = crosses(f, target(c, 0))

    @pl.when(early)
    def _():
        down_own(1 - k).wait_recv()
        send_down(order_down[:1])

    for q, group in enumerate(units):
        if q == max(0, slices - 1):
            @pl.when(early)
            def _():
                relay_lone()
                send_down(order_down[1:])

        for j, u in group:
            when_not(crosses(f, target(c, j)))(lambda: start_forward(c, j, u, 0))
            for s in range(1, chips):
                source = lax.rem(c + chips - s, chips)

                def pass_on():
                    exchanged(s, j, u).wait_recv()
                    start_forward(source, j, u, s)

                goes(source, j, u, s, pass_on)

    @when_not(early)
    def _():
        relay_lone()
        down_own(1 - k).wait_recv()
        send_down(order_down)

    source_core = lax.rem(f // blocks, 2)
    own_stays = source_core == k

    def arrive(shard, step):
        def arrival(count):
            held = half_rows(shard, k, 0, count)
            return remote(held, held, ps.at[0], frecv.at[shard], dev(c, f, 1 - k))

        if step in far:
            whole = jnp.logical_not(crosses(shard, f))
            for way in ways:
                pl.when(alone(shard, way))(lambda: arrival(half - lone[way]).wait_recv())
            rest = jnp.logical_or(whole, functools.reduce(jnp.logical_and, [offset != way for way in ways]))
            pl.when(rest)(lambda: arrival(half).wait_recv())
        elif step == 0:
            @when_not(own_stays)
            def _():
                arrival(half).wait_recv()
        else:
            arrival(half).wait_recv()

    def relay(shard, core):
        held = half_rows(shard, core)
        return remote(held, held, ps.at[0], pr.at[shard], dev(c, f, 1 - k))

    def accumulate(shard, first):
        weights = up_out[pl.ds(pl.multiple_of(shard * rows, rows), rows), :]
        product = jnp.dot(normed[shard], weights, preferred_element_type=jnp.float32)
        if first:
            acc[...] = product
        else:
            acc[...] += product

    near = shards // 2
    steps = list(range(1, near)) + [0] + list(range(near, shards))
    order = [flipped(f, s, shards) for s in steps]
    for position, shard in enumerate(order):
        arrive(shard, steps[position])
        relay(shard, k).start()
        if position > 0:
            before = order[position - 1]
            relay(before, 1 - k).wait_recv()
            accumulate(before, position == 1)
    relay(order[-1], 1 - k).wait_recv()
    accumulate(order[-1], False)
    hidden[...] = jnp.square(jnp.maximum(acc[...], 0.0)).astype(jnp.bfloat16)

    pieces = yr.shape[1]
    span = mixed.shape[0] // pieces

    def place(i):
        return pl.ds(i * span, span)

    def across(pair, i):
        at = place(i)
        return remote(
            part.at[2 * pair + 1 - y, at], ybuf.at[pair, at], ys.at[0], yr.at[pair, i],
            dev(c, z * 2 + 1 - y, k),
        )

    def along(pair, i):
        at = place(i)
        to = z + jnp.where(pair > z, 1, -1)
        slot = jnp.where(jnp.logical_and(pair < z, pair == to), pairs, pair)
        return remote(
            zout.at[pair, at], zin.at[slot, at], zs.at[0], zr.at[slot, i], dev(c, to * 2 + y, k)
        )

    def carried(slot, i):
        held = zin.at[slot, place(i)]
        return remote(held, held, zs.at[0], zr.at[slot, i], dev(c, f, k))

    def multiply(pair):
        both = jnp.dot(
            hidden[...], down_out[:, down_cols(pair)], preferred_element_type=jnp.float32
        ).astype(jnp.bfloat16)
        part[2 * pair] = both[:, :wide]
        part[2 * pair + 1] = both[:, wide:]
        for i in range(pieces):
            across(pair, i).start()

    def reduce(pair, some):
        inner = jnp.logical_and(pair != z, jnp.where(pair > z, z > 0, z < pairs - 1))
        outer = jnp.logical_and(pair != z, jnp.logical_not(inner))
        for i in some:
            at = place(i)

            def wide_of(ref, slot):
                return ref[slot, at].astype(jnp.float32)

            def summed():
                return wide_of(part, 2 * pair + y) + wide_of(ybuf, pair)

            across(pair, i).wait_recv()

            @pl.when(inner)
            def _():
                carried(pair, i).wait_recv()
                zout[pair, at] = (summed() + wide_of(zin, pair)).astype(jnp.bfloat16)
                along(pair, i).start()

            @pl.when(outer)
            def _():
                zout[pair, at] = summed().astype(jnp.bfloat16)
                along(pair, i).start()

            @pl.when(pair == z)
            def _():
                @pl.when(z == 0)
                def _():
                    carried(pairs, i).wait_recv()
                    mixed[at] = (summed() + wide_of(zin, pairs)).astype(jnp.bfloat16)

                @pl.when(z == pairs - 1)
                def _():
                    carried(pair, i).wait_recv()
                    mixed[at] = (summed() + wide_of(zin, pair)).astype(jnp.bfloat16)

                @pl.when(jnp.logical_and(z > 0, z < pairs - 1))
                def _():
                    carried(pair, i).wait_recv()
                    carried(pairs, i).wait_recv()
                    total = summed() + wide_of(zin, pair) + wide_of(zin, pairs)
                    mixed[at] = total.astype(jnp.bfloat16)

    def fetch(s, position):
        for i in range(chunks):
            down_arrival(s, position, i, xdr).wait_recv()
            down_relay(s, position, i).start()

    def fetched(s, position):
        for i in range(chunks):
            down_arrival(s, position, i, pdr).wait_recv()

    def pair_at(index):
        return pair_of(lax.rem(c + chips - index // 2, chips), lax.rem(index, 2))

    last = 2 * lax.rem(z // 2 + chips - c, chips) + 1
    home = last == 1

    def index_at(i):
        return last if i == pairs - 1 else i + jnp.where(i < last, 0, 1)

    sequence = [pair_at(index_at(i)) for i in range(pairs)]

    def begin(i):
        index = index_at(i)
        pl.when(index > 1)(lambda: fetch(index // 2, lax.rem(index, 2)))

    def complete(i):
        index = index_at(i)
        pl.when(index > 1)(lambda: fetched(index // 2, lax.rem(index, 2)))
        multiply(sequence[i])

    def take(i):
        if i > 0:
            begin(i)
            complete(i)
        else:
            multiply(sequence[i])

    def sent(source, semaphore):
        remote(source, source, semaphore, xr.at[0, 0, 0], dev(c, f, k)).wait_send()

    def gathered():
        down_own(k).wait_send()
        for way in ways:
            passed = (chips - 1) * (shards // 2) * lone[way]
            pl.when(offset == way)(lambda: sent(up_out.at[pl.ds(0, passed), :], msend.at[0]))
        sent(up_out.at[pl.ds(0, shards * half), :], ps.at[0])
        for s in range(chips):
            source = lax.rem(c + chips - s, chips)
            count = [piece * sum(pinned(u, s) == which for u in range(2 * slices)) for which in range(2)]
            for which in range(2):
                if not count[which]:
                    continue
                if s > 0:
                    def crossed():
                        sent(gath.at[0, pl.ds(0, count[which]), :], xs.at[s - 1, which])

                    if which:
                        when_not(crosses(f, target(c, 0)))(crossed)
                    else:
                        crossed()
                for j in range(blocks):
                    to = target(source, j)

                    def left(rows_left):
                        sent(gath.at[0, pl.ds(0, rows_left), pl.ds(0, block)], fsend.at[s, j, which])

                    gone = jnp.logical_not(crosses(f, to)) if which else to >= 0
                    pl.when(jnp.logical_and(gone, to != f))(lambda: left(count[which]))
                    pl.when(to == f)(lambda: left(count[which] // 2))

    def settle(i, first=0, end=pieces):
        reduce(sequence[i], range(first, end))

    outer = jnp.logical_or(z == 0, z == pairs - 1)
    own = pairs - 1
    take(0)
    take(1)
    gathered()

    @pl.when(jnp.logical_and(home, outer))
    def _():
        settle(0)
        for i in range(2, own):
            settle(i - 1, 0, EARLY_SUMS[0])
            begin(i)
            settle(i - 1, EARLY_SUMS[0], EARLY_SUMS[1])
            complete(i)
            settle(i - 1, EARLY_SUMS[1], pieces)
        take(own)

    @pl.when(jnp.logical_and(home, jnp.logical_not(outer)))
    def _():
        for i in range(2, pairs):
            take(i)
        if own == 3:
            for n in range(pieces):
                settle(0, n, n + 1)
                settle(1, n, n + 1)
        else:
            for i in range(own - 1):
                settle(i)

    @when_not(home)
    def _():
        for i in range(2, own):
            take(i)
        settle(0)

        @pl.when(outer)
        def _():
            settle(1, 0, LATE_SUMS)
            begin(own)
            settle(1, LATE_SUMS, pieces)

        when_not(outer)(lambda: begin(own))
        complete(own)
        when_not(outer)(lambda: settle(1))

        for i in range(2, own - 1):
            settle(i)

    settle(own - 1)
    settle(own)

    crossed = down_out.at[pl.ds(0, down_half), pl.ds(0, 2 * (chips - 1) * cols)]
    sent(crossed, xds.at[0])
    sent(crossed, pds.at[0])
    sent(part.at[pl.ds(0, pairs)], ys.at[0])
    sent(zout.at[pl.ds(0, pairs - 1)], zs.at[0])


def copy_kernel(up, down, mixed, up_out, down_out, mixed_out, sems):
    copies = []
    for index, (source, kept) in enumerate([(up, up_out), (down, down_out), (mixed, mixed_out)]):
        count = sems.shape[1]
        span = source.shape[0] // count
        for i in range(count):
            at = pl.ds(i * span, span)
            copies.append(pltpu.make_async_copy(source.at[at], kept.at[at], sems.at[index, i]))
    for copy in copies:
        copy.start()
    for copy in copies:
        copy.wait()


def per_device(gr, fs, tp, tokens, norm_gain, up_weight, down_weight):
    rows, width = up_weight.shape
    units, cols = down_weight.shape
    group = gr * tp
    chips = group // 2
    slices = max(1, rows // 2 // SLICE_ROWS)
    single = [slices * some // of if chips > 1 else 0 for some, of in SINGLE]
    block = width * group // fs
    blocks = width // block
    count, depth = tokens.shape
    model = cols * group
    pairs = fs // 2
    wide = model // fs
    assert pairs == group and pairs > 2 and pairs % blocks == 0
    others = max(1, chips - 1)
    vmem = pl.BlockSpec(memory_space=pltpu.VMEM)
    hbm = pl.BlockSpec(memory_space=pltpu.HBM)
    bf16, f32 = jnp.bfloat16, jnp.float32
    dma = pltpu.SemaphoreType.DMA
    results = (
        jax.ShapeDtypeStruct((depth, block), bf16),
        jax.ShapeDtypeStruct((units, model), bf16),
        jax.ShapeDtypeStruct((count, wide), bf16),
    )
    arrays = pl.pallas_call(
        functools.partial(fused_kernel, tp, blocks, fs, single),
        out_shape=results,
        in_specs=[hbm] * 4,
        out_specs=(vmem,) * 3,
        scratch_shapes=[
            pltpu.VMEM(tokens.shape, bf16),
            pltpu.VMEM((1, rows), f32),
            pltpu.VMEM(up_weight.shape, f32),
            pltpu.VMEM(down_weight.shape, f32),
            dma((4,)),
            pltpu.VMEM((chips, rows, width), bf16),
            pltpu.VMEM((fs, count, rows), bf16),
            pltpu.VMEM((count, block), f32),
            pltpu.VMEM((count, block), bf16),
            pltpu.VMEM((fs, count, wide), bf16),
            pltpu.VMEM((pairs, count, wide), bf16),
            pltpu.VMEM((pairs, count, wide), bf16),
            pltpu.VMEM((pairs + 1, count, wide), bf16),
            dma((others, 2)), dma((others, blocks, 2 * slices)), dma((chips, blocks, 2)), dma((2 * fs,)),
            dma((1,)), dma((1,)), dma((fs,)), dma((1,)), dma((1,)),
            dma((1,)), dma((others, 2, DOWN_CHUNKS)), dma((1,)), dma((others, 2, DOWN_CHUNKS)),
            dma((1,)), dma((pairs, PIECES)), dma((1,)), dma((pairs + 1, PIECES)),
        ],
        compiler_params=pltpu.CompilerParams(
            collective_id=0, has_side_effects=True, vmem_limit_bytes=FUSED_VMEM * MIB
        ),
        cost_estimate=pl.CostEstimate(
            flops=2 * count * block * (depth + model), bytes_accessed=160 * MIB, transcendentals=0
        ),
    )(*[pltpu.with_memory_space_constraint(x, pltpu.HBM) for x in (tokens, norm_gain[None, :], up_weight, down_weight)])
    return pl.pallas_call(
        copy_kernel,
        out_shape=results,
        in_specs=[vmem] * 3,
        out_specs=(hbm,) * 3,
        scratch_shapes=[dma((3, COPY_CHUNKS))],
        compiler_params=pltpu.CompilerParams(vmem_limit_bytes=COPY_VMEM * MIB),
        cost_estimate=pl.CostEstimate(flops=count * wide, bytes_accessed=18 * MIB, transcendentals=0),
    )(*arrays)


def solution(mesh):
    in_specs = (P(("gr", "tp"), None), P("fs"), P("fs", ("gr", "tp")), P("fs", ("gr", "tp")))
    out_specs = (P(None, "fs"), P("fs", None), P(("gr", "tp"), "fs"))
    body = functools.partial(per_device, mesh.shape["gr"], mesh.shape["fs"], mesh.shape["tp"])
    return jax.shard_map(
        body, mesh=mesh, in_specs=in_specs, out_specs=out_specs, check_vma=False
    )
```

```python
import functools

import jax
import jax.numpy as jnp
from jax import lax
from jax.experimental import pallas as pl
from jax.experimental.pallas import tpu as pltpu
from jax.sharding import PartitionSpec as P

MESH = pl.DeviceIdType.MESH
MIB = 1024 * 1024
FUSED_VMEM = 36
COPY_VMEM = 4
SLICE_ROWS = 32
SINGLE = ((1, 4), (1, 4))
PIECES = 4
DOWN_CHUNKS = 2
COPY_CHUNKS = 2
EARLY_SUMS = (1, 2)
LATE_SUMS = 3


def flipped(index, step, count):
    if count & (count - 1):
        return lax.rem(index + step, count)
    bit = 1
    while bit < count:
        if step & bit:
            index = index + (1 - 2 * lax.rem(index // bit, 2)) * bit
        bit *= 2
    return index


def remote(src, dst, send, recv, device):
    return pltpu.make_async_remote_copy(
        src_ref=src, dst_ref=dst, send_sem=send, recv_sem=recv,
        device_id=device, device_id_type=MESH,
    )


def when_not(condition):
    return pl.when(jnp.logical_not(condition))


def fused_kernel(
    tp, blocks, shards, single, tokens_in, gain_in, up_in, down_in, up_out, down_out, mixed,
    tokens, gain, up, down, loads, gath, normed, acc, hidden, part, ybuf, zout, zin,
    xs, xr, fsend, frecv, msend, ps, pr, ods, odr, xds, xdr, pds, pdr, ys, yr, zs, zr,
):
    load = [
        pltpu.make_async_copy(source, kept, loads.at[i])
        for i, (source, kept) in enumerate(
            [(gain_in, gain), (up_in, up), (down_in, down), (tokens_in, tokens)]
        )
    ]
    for copy in load:
        copy.start()
    g, f, t = lax.axis_index("gr"), lax.axis_index("fs"), lax.axis_index("tp")
    per = tp // 2
    chips = gath.shape[0]
    c, k = g * per + t // 2, lax.rem(t, 2)
    rows, width = up.shape
    half = rows // 2
    block = width // blocks
    cols = down.shape[1]
    pairs = ybuf.shape[0]
    wide = mixed.shape[1]
    z, y = f // 2, lax.rem(f, 2)

    def dev(chip, shard, core):
        return (chip // per, shard, lax.rem(chip, per) * 2 + core)

    def down_cols(pair):
        return pl.ds(pl.multiple_of(pair * cols, cols), cols)

    barrier = pltpu.get_barrier_semaphore()
    for s in range(1, chips):
        pl.semaphore_signal(
            barrier, inc=1, device_id=dev(lax.rem(c + s, chips), f, k), device_id_type=MESH
        )
    for s in range(shards):
        for core in range(2):
            if s == 0 and core == 0:
                continue
            other = lax.rem(f + s, shards)
            core_id = lax.rem(k + core, 2)
            pl.semaphore_signal(
                barrier, inc=1, device_id=dev(c, other, core_id), device_id_type=MESH
            )

    load[0].wait()
    square = (rows, rows)
    diagonal = lax.broadcasted_iota(jnp.int32, square, 0) == lax.broadcasted_iota(jnp.int32, square, 1)
    column = jnp.sum(jnp.where(diagonal, gain[...], 0.0), axis=1, keepdims=True)
    load[1].wait()
    gath[c] = (column * up[...]).astype(jnp.bfloat16)
    pl.semaphore_wait(barrier, chips - 1 + 2 * shards - 1)

    slices = xr.shape[2] // 2
    piece = half // slices

    def route(u):
        q = u % slices
        return 1 if q < single[1] else 0 if q < sum(single) else None

    def crosses(source, target):
        return source // (shards // 2) != target // (shards // 2)

    def unit(chip, j, u):
        return gath.at[chip, pl.ds(u * piece, piece), pl.ds(j * block, block)]

    def half_rows(shard, core, first=0, count=half):
        at = pl.multiple_of(shard * rows + core * half + first, piece)
        return up_out.at[pl.ds(at, count), :]

    def target(chip, j):
        return (chip * 2 + k) * blocks + j

    def landing(u):
        return up_out.at[pl.ds(pl.multiple_of(f * rows + u * piece, piece), piece), :]

    def stays(chip, j, u):
        return jnp.logical_and(target(chip, j) == f, k == u // slices)

    def pinned(u, s):
        return 0 if route(u) in (None, s) else 1

    def forward(chip, j, u, s):
        to = target(chip, j)
        at = f if route(u) is None else f + jnp.where(crosses(f, to), shards, 0)
        return remote(
            unit(chip, j, u), landing(u), fsend.at[s, j, pinned(u, s)], frecv.at[at],
            dev(c, to, u // slices),
        )

    def start_forward(chip, j, u, s):
        @when_not(stays(chip, j, u))
        def _():
            forward(chip, j, u, s).start()

        @pl.when(stays(chip, j, u))
        def _():
            landing(u)[...] = unit(chip, j, u)[...]

    def goes(chip, j, u, offset, action):
        if route(u) is None or route(u) == offset:
            action()
        else:
            when_not(crosses(f, target(chip, j)))(action)

    def exchange(s, j, u):
        return remote(
            unit(c, j, u), unit(c, j, u), xs.at[s - 1, pinned(u, s)], xr.at[s - 1, j, u],
            dev(lax.rem(c + s, chips), f, k),
        )

    def exchanged(s, j, u):
        source = lax.rem(c + chips - s, chips)
        return remote(
            unit(source, j, u), unit(source, j, u), xs.at[s - 1, 0], xr.at[s - 1, j, u], dev(c, f, k)
        )

    units = [
        [(j, q + core * slices) for core in range(2) for j in range(blocks)] for q in range(slices)
    ]
    for group in units:
        for j, u in group:
            for s in range(1, chips):
                goes(c, j, u, s, lambda: exchange(s, j, u).start())
            if route(u) in (None, 0):
                pl.when(crosses(f, target(c, j)))(lambda: forward(c, j, u, 0).start())

    load[2].wait()
    own_pair = c * 2 + k
    down_out[:, down_cols(own_pair)] = down[...].astype(jnp.bfloat16)
    down_half = down.shape[0] // 2
    chunks = xdr.shape[2]
    chunk = down_half // chunks

    def down_own(core):
        held = down_out.at[:, down_cols(c * 2 + core)]
        return remote(held, held, ods.at[0], odr.at[0], dev(c, f, 1 - k))

    down_own(k).start()

    def pair_of(chip, position):
        low = 2 * chip
        return low + jnp.where(z <= low, 1 - position, position)

    def down_piece(pair, core, i):
        at = pl.multiple_of(core * down_half + i * chunk, chunk)
        return down_out.at[pl.ds(at, chunk), down_cols(pair)]

    def down_across(s, position, i):
        held = down_piece(pair_of(c, position), k, i)
        return remote(
            held, held, xds.at[0], xdr.at[s - 1, position, i], dev(lax.rem(c + s, chips), f, k)
        )

    def down_relay(s, position, i):
        held = down_piece(pair_of(lax.rem(c + chips - s, chips), position), k, i)
        return remote(held, held, pds.at[0], pdr.at[s - 1, position, i], dev(c, f, 1 - k))

    def down_arrival(s, position, i, semaphore):
        held = down_piece(0, k, i)
        return remote(held, held, xds.at[0], semaphore.at[s - 1, position, i], dev(c, f, k))

    load[3].wait()
    widened = tokens[...].astype(jnp.float32)
    scale = lax.rsqrt(jnp.mean(widened * widened, axis=-1, keepdims=True) + 1e-06)
    for shard in range(shards):
        share = tokens[:, shard * rows:(shard + 1) * rows].astype(jnp.float32)
        normed[shard] = (share * scale).astype(jnp.bfloat16)

    owner = f // (2 * blocks)
    offset = lax.rem(c + chips - owner, chips)
    lone = [count * piece for count in single]

    def alone(shard, way):
        return jnp.logical_and(crosses(shard, f), offset == way)

    def lone_rows(shard, way):
        return half_rows(shard, k, lone[1] if way == 0 else 0, lone[way])

    def lone_arrival(shard, way):
        held = lone_rows(shard, way)
        return remote(held, held, msend.at[0], frecv.at[shards + shard], dev(c, f, k))

    def lone_relay(shard, way, s):
        held = lone_rows(shard, way)
        return remote(
            held, held, msend.at[0], frecv.at[shard], dev(lax.rem(c + s, chips), f, k)
        )

    ways = [way for way in range(2) if single[way]]
    even = not shards & (shards - 1)
    far = [s for s in range(1, shards) if sum(single) and (not even or s & (shards // 2))]

    def relay_lone():
        for step in far:
            shard = flipped(f, step, shards)

            for way in ways:
                @pl.when(alone(shard, way))
                def _():
                    lone_arrival(shard, way).wait_recv()
                    for s in range(1, chips):
                        lone_relay(shard, way, s).start()

    order_down = [(position, i) for position in range(2) for i in range(chunks)]

    def send_down(pieces_of):
        for position, i in pieces_of:
            for s in range(1, chips):
                down_across(s, position, i).start()

    early = crosses(f, target(c, 0))

    @pl.when(early)
    def _():
        down_own(1 - k).wait_recv()
        send_down(order_down[:1])

    for q, group in enumerate(units):
        if q == max(0, slices - 1):
            @pl.when(early)
            def _():
                relay_lone()
                send_down(order_down[1:])

        for j, u in group:
            when_not(crosses(f, target(c, j)))(lambda: start_forward(c, j, u, 0))
            for s in range(1, chips):
                source = lax.rem(c + chips - s, chips)

                def pass_on():
                    exchanged(s, j, u).wait_recv()
                    start_forward(source, j, u, s)

                goes(source, j, u, s, pass_on)

    @when_not(early)
    def _():
        relay_lone()
        down_own(1 - k).wait_recv()
        send_down(order_down)

    source_core = lax.rem(f // blocks, 2)
    own_stays = source_core == k

    def arrive(shard, step):
        def arrival(count):
            held = half_rows(shard, k, 0, count)
            return remote(held, held, ps.at[0], frecv.at[shard], dev(c, f, 1 - k))

        if step in far:
            whole = jnp.logical_not(crosses(shard, f))
            for way in ways:
                pl.when(alone(shard, way))(lambda: arrival(half - lone[way]).wait_recv())
            rest = jnp.logical_or(whole, functools.reduce(jnp.logical_and, [offset != way for way in ways]))
            pl.when(rest)(lambda: arrival(half).wait_recv())
        elif step == 0:
            @when_not(own_stays)
            def _():
                arrival(half).wait_recv()
        else:
            arrival(half).wait_recv()

    def relay(shard, core):
        held = half_rows(shard, core)
        return remote(held, held, ps.at[0], pr.at[shard], dev(c, f, 1 - k))

    def accumulate(shard, first):
        weights = up_out[pl.ds(pl.multiple_of(shard * rows, rows), rows), :]
        product = jnp.dot(normed[shard], weights, preferred_element_type=jnp.float32)
        if first:
            acc[...] = product
        else:
            acc[...] += product

    near = shards // 2
    steps = list(range(1, near)) + [0] + list(range(near, shards))
    order = [flipped(f, s, shards) for s in steps]
    for position, shard in enumerate(order):
        arrive(shard, steps[position])
        relay(shard, k).start()
        if position > 0:
            before = order[position - 1]
            relay(before, 1 - k).wait_recv()
            accumulate(before, position == 1)
    relay(order[-1], 1 - k).wait_recv()

    pieces = yr.shape[1]
    span = mixed.shape[0] // pieces

    def place(i):
        return pl.ds(i * span, span)

    def across(pair, i):
        at = place(i)
        return remote(
            part.at[2 * pair + 1 - y, at], ybuf.at[pair, at], ys.at[0], yr.at[pair, i],
            dev(c, z * 2 + 1 - y, k),
        )

    def along(pair, i):
        at = place(i)
        to = z + jnp.where(pair > z, 1, -1)
        slot = jnp.where(jnp.logical_and(pair < z, pair == to), pairs, pair)
        return remote(
            zout.at[pair, at], zin.at[slot, at], zs.at[0], zr.at[slot, i], dev(c, to * 2 + y, k)
        )

    def carried(slot, i):
        held = zin.at[slot, place(i)]
        return remote(held, held, zs.at[0], zr.at[slot, i], dev(c, f, k))

    def multiply(pair, first=0, end=None):
        end = pieces if end is None else end
        at = pl.ds(first * span, (end - first) * span)
        both = jnp.dot(
            hidden[at], down_out[:, down_cols(pair)], preferred_element_type=jnp.float32
        ).astype(jnp.bfloat16)
        part[2 * pair, at] = both[:, :wide]
        part[2 * pair + 1, at] = both[:, wide:]
        for i in range(first, end):
            across(pair, i).start()

    def reduce(pair, some):
        inner = jnp.logical_and(pair != z, jnp.where(pair > z, z > 0, z < pairs - 1))
        outer = jnp.logical_and(pair != z, jnp.logical_not(inner))
        for i in some:
            at = place(i)

            def wide_of(ref, slot):
                return ref[slot, at].astype(jnp.float32)

            def summed():
                return wide_of(part, 2 * pair + y) + wide_of(ybuf, pair)

            across(pair, i).wait_recv()

            @pl.when(inner)
            def _():
                carried(pair, i).wait_recv()
                zout[pair, at] = (summed() + wide_of(zin, pair)).astype(jnp.bfloat16)
                along(pair, i).start()

            @pl.when(outer)
            def _():
                zout[pair, at] = summed().astype(jnp.bfloat16)
                along(pair, i).start()

            @pl.when(pair == z)
            def _():
                @pl.when(z == 0)
                def _():
                    carried(pairs, i).wait_recv()
                    mixed[at] = (summed() + wide_of(zin, pairs)).astype(jnp.bfloat16)

                @pl.when(z == pairs - 1)
                def _():
                    carried(pair, i).wait_recv()
                    mixed[at] = (summed() + wide_of(zin, pair)).astype(jnp.bfloat16)

                @pl.when(jnp.logical_and(z > 0, z < pairs - 1))
                def _():
                    carried(pair, i).wait_recv()
                    carried(pairs, i).wait_recv()
                    total = summed() + wide_of(zin, pair) + wide_of(zin, pairs)
                    mixed[at] = total.astype(jnp.bfloat16)

    def fetch(s, position):
        for i in range(chunks):
            down_arrival(s, position, i, xdr).wait_recv()
            down_relay(s, position, i).start()

    def fetched(s, position):
        for i in range(chunks):
            down_arrival(s, position, i, pdr).wait_recv()

    def pair_at(index):
        return pair_of(lax.rem(c + chips - index // 2, chips), lax.rem(index, 2))

    last = 2 * lax.rem(z // 2 + chips - c, chips) + 1
    home = last == 1

    def index_at(i):
        return last if i == pairs - 1 else i + jnp.where(i < last, 0, 1)

    sequence = [pair_at(index_at(i)) for i in range(pairs)]

    def begin(i):
        index = index_at(i)
        pl.when(index > 1)(lambda: fetch(index // 2, lax.rem(index, 2)))

    def complete(i):
        index = index_at(i)
        pl.when(index > 1)(lambda: fetched(index // 2, lax.rem(index, 2)))
        multiply(sequence[i])

    def take(i):
        if i > 0:
            begin(i)
            complete(i)
        else:
            multiply(sequence[i])

    def sent(source, semaphore):
        remote(source, source, semaphore, xr.at[0, 0, 0], dev(c, f, k)).wait_send()

    def gathered():
        down_own(k).wait_send()
        for way in ways:
            passed = (chips - 1) * (shards // 2) * lone[way]
            pl.when(offset == way)(lambda: sent(up_out.at[pl.ds(0, passed), :], msend.at[0]))
        sent(up_out.at[pl.ds(0, shards * half), :], ps.at[0])
        for s in range(chips):
            source = lax.rem(c + chips - s, chips)
            count = [piece * sum(pinned(u, s) == which for u in range(2 * slices)) for which in range(2)]
            for which in range(2):
                if not count[which]:
                    continue
                if s > 0:
                    def crossed():
                        sent(gath.at[0, pl.ds(0, count[which]), :], xs.at[s - 1, which])

                    if which:
                        when_not(crosses(f, target(c, 0)))(crossed)
                    else:
                        crossed()
                for j in range(blocks):
                    to = target(source, j)

                    def left(rows_left):
                        sent(gath.at[0, pl.ds(0, rows_left), pl.ds(0, block)], fsend.at[s, j, which])

                    gone = jnp.logical_not(crosses(f, to)) if which else to >= 0
                    pl.when(jnp.logical_and(gone, to != f))(lambda: left(count[which]))
                    pl.when(to == f)(lambda: left(count[which] // 2))

    def settle(i, first=0, end=pieces):
        reduce(sequence[i], range(first, end))

    outer = jnp.logical_or(z == 0, z == pairs - 1)
    own = pairs - 1
    final = up_out.at[pl.ds(pl.multiple_of(order[-1] * rows, rows), rows), :]
    for first in range(0, pieces, pieces // 2):
        end = first + pieces // 2
        at = pl.ds(first * span, (end - first) * span)
        product = jnp.dot(normed[order[-1], at], final[...], preferred_element_type=jnp.float32)
        hidden[at] = jnp.square(jnp.maximum(acc[at] + product, 0.0)).astype(jnp.bfloat16)
        multiply(sequence[0], first, end)
    take(1)
    gathered()

    @pl.when(jnp.logical_and(home, outer))
    def _():
        settle(0)
        for i in range(2, own):
            settle(i - 1, 0, EARLY_SUMS[0])
            begin(i)
            settle(i - 1, EARLY_SUMS[0], EARLY_SUMS[1])
            complete(i)
            settle(i - 1, EARLY_SUMS[1], pieces)
        take(own)

    @pl.when(jnp.logical_and(home, jnp.logical_not(outer)))
    def _():
        for i in range(2, pairs):
            take(i)
        if own == 3:
            for n in range(pieces):
                settle(0, n, n + 1)
                settle(1, n, n + 1)
        else:
            for i in range(own - 1):
                settle(i)

    @when_not(home)
    def _():
        for i in range(2, own):
            take(i)
        settle(0)

        @pl.when(outer)
        def _():
            settle(1, 0, LATE_SUMS)
            begin(own)
            settle(1, LATE_SUMS, pieces)

        when_not(outer)(lambda: begin(own))
        complete(own)
        when_not(outer)(lambda: settle(1))

        for i in range(2, own - 1):
            settle(i)

    settle(own - 1)
    settle(own)

    crossed = down_out.at[pl.ds(0, down_half), pl.ds(0, 2 * (chips - 1) * cols)]
    sent(crossed, xds.at[0])
    sent(crossed, pds.at[0])
    sent(part.at[pl.ds(0, pairs)], ys.at[0])
    sent(zout.at[pl.ds(0, pairs - 1)], zs.at[0])


def copy_kernel(up, down, mixed, up_out, down_out, mixed_out, sems):
    copies = []
    for index, (source, kept) in enumerate([(up, up_out), (down, down_out), (mixed, mixed_out)]):
        count = sems.shape[1]
        span = source.shape[0] // count
        for i in range(count):
            at = pl.ds(i * span, span)
            copies.append(pltpu.make_async_copy(source.at[at], kept.at[at], sems.at[index, i]))
    for copy in copies:
        copy.start()
    for copy in copies:
        copy.wait()


def per_device(gr, fs, tp, tokens, norm_gain, up_weight, down_weight):
    rows, width = up_weight.shape
    units, cols = down_weight.shape
    group = gr * tp
    chips = group // 2
    slices = max(1, rows // 2 // SLICE_ROWS)
    single = [slices * some // of if chips > 1 else 0 for some, of in SINGLE]
    block = width * group // fs
    blocks = width // block
    count, depth = tokens.shape
    model = cols * group
    pairs = fs // 2
    wide = model // fs
    assert pairs == group and pairs > 2 and pairs % blocks == 0
    others = max(1, chips - 1)
    vmem = pl.BlockSpec(memory_space=pltpu.VMEM)
    hbm = pl.BlockSpec(memory_space=pltpu.HBM)
    bf16, f32 = jnp.bfloat16, jnp.float32
    dma = pltpu.SemaphoreType.DMA
    results = (
        jax.ShapeDtypeStruct((depth, block), bf16),
        jax.ShapeDtypeStruct((units, model), bf16),
        jax.ShapeDtypeStruct((count, wide), bf16),
    )
    arrays = pl.pallas_call(
        functools.partial(fused_kernel, tp, blocks, fs, single),
        out_shape=results,
        in_specs=[hbm] * 4,
        out_specs=(vmem,) * 3,
        scratch_shapes=[
            pltpu.VMEM(tokens.shape, bf16),
            pltpu.VMEM((1, rows), f32),
            pltpu.VMEM(up_weight.shape, f32),
            pltpu.VMEM(down_weight.shape, f32),
            dma((4,)),
            pltpu.VMEM((chips, rows, width), bf16),
            pltpu.VMEM((fs, count, rows), bf16),
            pltpu.VMEM((count, block), f32),
            pltpu.VMEM((count, block), bf16),
            pltpu.VMEM((fs, count, wide), bf16),
            pltpu.VMEM((pairs, count, wide), bf16),
            pltpu.VMEM((pairs, count, wide), bf16),
            pltpu.VMEM((pairs + 1, count, wide), bf16),
            dma((others, 2)), dma((others, blocks, 2 * slices)), dma((chips, blocks, 2)), dma((2 * fs,)),
            dma((1,)), dma((1,)), dma((fs,)), dma((1,)), dma((1,)),
            dma((1,)), dma((others, 2, DOWN_CHUNKS)), dma((1,)), dma((others, 2, DOWN_CHUNKS)),
            dma((1,)), dma((pairs, PIECES)), dma((1,)), dma((pairs + 1, PIECES)),
        ],
        compiler_params=pltpu.CompilerParams(
            collective_id=0, has_side_effects=True, vmem_limit_bytes=FUSED_VMEM * MIB
        ),
        cost_estimate=pl.CostEstimate(
            flops=2 * count * block * (depth + model), bytes_accessed=160 * MIB, transcendentals=0
        ),
    )(*[pltpu.with_memory_space_constraint(x, pltpu.HBM) for x in (tokens, norm_gain[None, :], up_weight, down_weight)])
    return pl.pallas_call(
        copy_kernel,
        out_shape=results,
        in_specs=[vmem] * 3,
        out_specs=(hbm,) * 3,
        scratch_shapes=[dma((3, COPY_CHUNKS))],
        compiler_params=pltpu.CompilerParams(vmem_limit_bytes=COPY_VMEM * MIB),
        cost_estimate=pl.CostEstimate(flops=count * wide, bytes_accessed=18 * MIB, transcendentals=0),
    )(*arrays)


def solution(mesh):
    in_specs = (P(("gr", "tp"), None), P("fs"), P("fs", ("gr", "tp")), P("fs", ("gr", "tp")))
    out_specs = (P(None, "fs"), P("fs", None), P(("gr", "tp"), "fs"))
    body = functools.partial(per_device, mesh.shape["gr"], mesh.shape["fs"], mesh.shape["tp"])
    return jax.shard_map(
        body, mesh=mesh, in_specs=in_specs, out_specs=out_specs, check_vma=False
    )
```
